32 devices in a mesh: grp: 2 (over y), ep: 4 (over z), tp: 4 (over x, core).
Axes of the slice: x: 2, y: 2, z: 4, core: 2. Of those that a mesh axis runs over, the one named last changes fastest.
Arguments:
- conv_x: bfloat16 [8192, 2048], P(('grp', 'ep', 'tp')), parts along dimension 0, may hold values from -6 to 6
- conv_c: bfloat16 [8192, 2048], P(('grp', 'ep', 'tp')), parts along dimension 0, may hold values from -6 to 6
- conv_b: bfloat16 [8192, 2048], P(('grp', 'ep', 'tp')), parts along dimension 0, may hold values from -6 to 6
- conv_taps: float32 [3, 2048], replicated, may hold values from -3.5 to 3.5
- w_out: bfloat16 [2048, 2048], P('tp'), may hold values from -0.125 to 0.125
- tokens_b: bfloat16 [4096, 2048], P(('grp', 'ep', 'tp')), parts along dimension 0, may hold values from -6 to 6
- norm_gain: float32 [2048], replicated, may hold values from 0.1 to 1.9
- route_b: int32 [4096, 2], P(('grp', 'ep', 'tp')), parts along dimension 0, may hold values from 0 to 3, all different within a row; in each aligned block of 128 rows (0 to 127, 128 to 255, ...) at most 128 rows name the same one
- route_weights: float32 [4096, 2], P(('grp', 'ep', 'tp')), parts along dimension 0, may hold values from 0.1 to 1
- w_gate: bfloat16 [4, 2048, 1024], P('ep', None, 'tp'), may hold values from -0.125 to 0.125
- w_up: bfloat16 [4, 2048, 1024], P('ep', None, 'tp'), may hold values from -0.125 to 0.125
- w_down: bfloat16 [4, 1024, 2048], P('ep', 'tp'), may hold values from -0.1875 to 0.1875
Outputs:
- mixed_a: bfloat16 [8192, 2048], P(('grp', 'ep', 'tp')), parts along dimension 0
- experts_b: bfloat16 [4096, 2048], P(('grp', 'ep', 'tp')), parts along dimension 0
The draws below stay inside these ranges and needn't reach their ends.
There are 2 independent parts, one for each index of `grp`. The reference program is written for one: setup_inputs(seed, part) draws one part's arguments, and reference() takes and returns one part's arrays. A program takes and returns all parts, laid end to end along the dimension named above; an argument that names none is the same for every part. Nothing has to cross between parts.
Inputs may be any that keep to these rules, and one draw needn't show every extreme that they name: `route_b`: the 2 experts of a row differ. Within the 128 rows of one device no expert is named more than 128 times, and in every draw some device names some expert exactly 128 times.
All inputs are finite; a program needn't handle non-finite values.
Results may differ from the reference program's by a relative error of at most 0.012.
Values may be sent and summed in bfloat16 or wider, within the bound.
A program may use at most 128 MiB of HBM per device.

```python
import math
import jax
import jax.numpy as jnp
import numpy as np
from jax import lax

D = 2048
CH = 2048
CONV = 3
FF = 1024
TOPK = 2
ROWS_B = 128
EXPERTS = 4
CAP = 128
SEQ = 4096
TOKENS_B = 2048
N_EP = 4
N_TP = 4


def steps_of(stream_key, shape, cuts, low, high):
    factor_of = 1.0
    for axis_at, blocks in cuts:
        draws = jax.random.uniform(jax.random.fold_in(jax.random.fold_in(stream_key, 6), axis_at), (blocks,), jnp.float32, low / len(cuts), high / len(cuts))
        factor_of = factor_of * jnp.repeat(jnp.exp(draws), shape[axis_at] // blocks).reshape((-1,) + (1,) * (len(shape) - 1 - axis_at))
    return factor_of


def assign_block(stream_key, own, number, rows, count, top, bound, slope):
    sequence = jax.random.permutation(stream_key, count)
    heavy_load, usual = portions_of(count, rows * top, bound, slope, True), portions_of(count, rows * top, bound, slope, False)
    places = jnp.arange(count)

    def named(tallies, offset_by):
        used = int((tallies > 0).sum())
        fixed = max(1, used // 4)
        shifted = fixed + (places - fixed + offset_by * (used - fixed)) % max(1, count - fixed)
        return jnp.zeros((count,), jnp.int32).at[sequence[jnp.where(places < fixed, places, shifted)]].set(jnp.asarray(tallies, jnp.int32))

    tallies = jnp.where(number % 4 == 0, named(heavy_load, number // 4), named(usual, number - number // 4 - 1))
    mixed = jax.random.permutation(jax.random.fold_in(own, 3), count)
    giver, sink = mixed[0:count // 2 * 2:2], mixed[1:count // 2 * 2:2]
    slack = jnp.minimum(tallies[giver] - 1, bound - tallies[sink]) // 2
    slack = jnp.where((giver == sequence[0]) | (sink == sequence[0]) | (tallies[sink] == 0), 0, jnp.maximum(slack, 0))
    shifted = jax.random.randint(jax.random.fold_in(own, 4), (count // 2,), 0, 1 << 20) % (slack + 1)
    tallies = tallies.at[giver].add(-shifted).at[sink].add(shifted)
    members = jnp.searchsorted(jnp.cumsum(tallies), jnp.arange(rows * top), side="right").astype(jnp.int32)
    table = members.reshape(top, rows).T
    table = table[jax.random.permutation(jax.random.fold_in(own, 1), rows)]
    offset_by = jax.random.randint(jax.random.fold_in(own, 2), (rows, 1), 0, top)
    return jnp.take_along_axis(table, (jnp.arange(top)[None, :] + offset_by) % top, axis=1)


def portions_of(count, total, most, lean, full):
    weights = [(1 << 20) // math.isqrt(standing ** lean) + 1 for standing in range(1, count + 1)]
    largest = most if full else min(most, max(-(-total // count), total * weights[0] // sum(weights)))
    least = 1 if total - largest >= count - 1 else 0
    counts, rest = [largest] + [least] * (count - 1), total - largest - least * (count - 1)
    while rest > 0:
        candidates = [i for i in range(1, count) if counts[i] < largest] or [i for i in range(1, count) if counts[i] < most]
        mass, left = sum([weights[i] for i in candidates]), rest
        for i in candidates:
            addition = min(most - counts[i], max(1, left * weights[i] // mass), rest)
            counts[i] = counts[i] + addition
            rest = rest - addition
    return np.array(counts)


def bell_draw(key, dims, spread, most, cuts=(), kind=jnp.bfloat16):
    entries = spread * jax.random.normal(key, dims, jnp.float32)
    if cuts:
        entries = entries * steps_of(key, dims, cuts, -0.22, 0.18)
    return jnp.clip(entries, -most, most).astype(kind)


def setup_inputs(seed: int = 0, part: int = 0) -> dict:
    streams_of = jax.random.split(jax.random.key(seed), 13)
    own_keys = jax.random.split(jax.random.fold_in(streams_of[12], part), 13)
    conv_x = bell_draw(own_keys[0], (SEQ, CH), 1.0, 6.0, ((0, 16),))
    conv_c = bell_draw(own_keys[1], (SEQ, CH), 1.0, 6.0, ((0, 16),))
    conv_b = bell_draw(own_keys[2], (SEQ, CH), 1.0, 6.0, ((0, 16),))
    conv_taps = bell_draw(streams_of[3], (CONV, CH), CONV ** -0.5, 3.5, (), jnp.float32)
    w_out = bell_draw(streams_of[4], (CH, D), CH ** -0.5, 0.125, ((0, 4),))
    tokens_b = bell_draw(own_keys[5], (TOKENS_B, D), 1.0, 6.0, ((0, 16),))
    norm_gain = jnp.clip(1.0 + 0.18 * jax.random.normal(streams_of[6], (D,), jnp.float32), 0.1, 1.9)
    route_b_keys = jax.random.split(jax.random.fold_in(own_keys[7], 1), TOKENS_B // ROWS_B)
    route_b_turns = jax.random.permutation(jax.random.fold_in(own_keys[7], 3), TOKENS_B // ROWS_B)
    route_b = jax.vmap(lambda own, number: assign_block(jax.random.fold_in(own_keys[7], 2), own, number, ROWS_B, EXPERTS, TOPK, CAP, 2))(route_b_keys, route_b_turns).reshape((TOKENS_B, TOPK))
    route_weights = jnp.clip(jnp.exp(math.log(1.0) - 2.3025851 * jax.random.uniform(own_keys[8], (TOKENS_B, TOPK), jnp.float32) ** steps_of(own_keys[8], (TOKENS_B, TOPK), ((0, 16),), -0.2, 0.2)), 0.1, 1.0)
    w_gate = bell_draw(streams_of[9], (EXPERTS, D, FF), D ** -0.5, 0.125, ((0, 4), (2, 4)))
    w_up = bell_draw(streams_of[10], (EXPERTS, D, FF), D ** -0.5, 0.125, ((0, 4), (2, 4)))
    w_down = bell_draw(streams_of[11], (EXPERTS, FF, D), FF ** -0.5, 0.1875, ((0, 4), (1, 4)))
    return {"conv_x": conv_x, "conv_c": conv_c, "conv_b": conv_b, "conv_taps": conv_taps, "w_out": w_out, "tokens_b": tokens_b, "norm_gain": norm_gain, "route_b": route_b, "route_weights": route_weights, "w_gate": w_gate, "w_up": w_up, "w_down": w_down}


def slot_ranks(route):
    flat = route.reshape(-1)
    onehot = (flat[:, None] == jnp.arange(EXPERTS, dtype=jnp.int32)[None, :]).astype(jnp.int32)
    earlier = jnp.cumsum(onehot, axis=0) - onehot
    return lax.optimization_barrier(jnp.sum(earlier * onehot, axis=1)).reshape(route.shape)

def reference(conv_x, conv_c, conv_b, conv_taps, w_out, tokens_b, norm_gain, route_b, route_weights, w_gate, w_up, w_down):
    mixed_u = (conv_c.astype(jnp.float32) * conv_x.astype(jnp.float32)).astype(jnp.bfloat16)
    extended = jnp.concatenate([jnp.zeros((CONV - 1, CH), jnp.bfloat16), mixed_u], axis=0)
    filtered = jnp.zeros((SEQ, CH), jnp.float32)
    for shift_tap in range(CONV):
        filtered = filtered + conv_taps[shift_tap][None, :] * extended[shift_tap:shift_tap + SEQ].astype(jnp.float32)
    gated = (conv_b.astype(jnp.float32) * filtered).astype(jnp.bfloat16)
    mixed_a = jnp.dot(gated, w_out, preferred_element_type=jnp.float32).astype(jnp.bfloat16)
    tokens_f = tokens_b.astype(jnp.float32)
    normed = (tokens_f * lax.rsqrt(lax.optimization_barrier(jnp.mean(tokens_f * tokens_f, axis=-1, keepdims=True)) + 1e-06) * norm_gain).astype(jnp.bfloat16)
    sources = N_EP * N_TP
    slots = jax.vmap(slot_ranks)(route_b.reshape(sources, ROWS_B, TOPK)).reshape(TOKENS_B, TOPK)
    source_id = (jnp.arange(TOKENS_B, dtype=jnp.int32) // ROWS_B)[:, None]
    position = source_id * CAP + slots
    token_id = jnp.broadcast_to(jnp.arange(TOKENS_B, dtype=jnp.int32)[:, None], (TOKENS_B, TOPK))
    fill_table = jnp.full((EXPERTS, sources * CAP), TOKENS_B, jnp.int32)
    fill_table = fill_table.at[route_b.reshape(-1), position.reshape(-1)].set(token_id.reshape(-1))
    padded = jnp.concatenate([normed, jnp.zeros((1, D), jnp.bfloat16)], axis=0)

    def one_expert(operands):
        fill_row, gate_w, up_w, down_w = operands
        rows = padded[fill_row]
        gate_val = jnp.dot(rows, gate_w, preferred_element_type=jnp.float32)
        up_val = jnp.dot(rows, up_w, preferred_element_type=jnp.float32)
        hidden = (jax.nn.silu(gate_val) * up_val).astype(jnp.bfloat16)
        blocks = hidden.reshape(-1, N_TP, FF // N_TP).astype(jnp.float32)
        down_blocks = down_w.reshape(N_TP, FF // N_TP, D).astype(jnp.float32)
        partial_sums = jnp.einsum('rqf,qfd->qrd', blocks, down_blocks).astype(jnp.bfloat16)
        partial_sums = lax.optimization_barrier(partial_sums)
        return lax.optimization_barrier(jnp.sum(partial_sums.astype(jnp.float32), axis=0)).astype(jnp.bfloat16)
    results = lax.map(one_expert, (fill_table, w_gate, w_up, w_down))
    flat_results = results.reshape(EXPERTS * sources * CAP, D)
    picked = flat_results[route_b * (sources * CAP) + position]
    shares = route_weights / lax.optimization_barrier(jnp.sum(route_weights, axis=-1, keepdims=True))
    experts_b = lax.optimization_barrier(jnp.sum(picked.astype(jnp.float32) * shares[:, :, None], axis=1)).astype(jnp.bfloat16)
    return (mixed_a, experts_b)
```

```python
import functools
import jax
import jax.numpy as jnp
from jax import lax
from jax.experimental import pallas as pl
from jax.experimental.pallas import tpu as pltpu
from jax.sharding import PartitionSpec as P

D = 2048
TOPK = 2


def shifted(x, axis, by):
    size = lax.axis_size(axis)
    pairs = [(i, i + by) for i in range(size) if 0 <= i + by < size]
    return lax.ppermute(x, axis, pairs)


def slot_targets(route, experts, capacity):
    flat = route.reshape(-1)
    onehot = (flat[:, None] == jnp.arange(experts, dtype=jnp.int32)[None, :]).astype(jnp.int32)
    earlier = jnp.cumsum(onehot, axis=0) - onehot
    ranks = jnp.sum(earlier * onehot, axis=1).reshape(route.shape)
    return route * capacity + ranks


def fill_slots(targets, slot_total, filler):
    token_ids = jnp.repeat(jnp.arange(filler, dtype=jnp.int32), targets.shape[1])
    return jnp.full((slot_total,), filler, jnp.int32).at[targets.reshape(-1)].set(token_ids)


def expert_hidden(rows, weight_gate, weight_up):
    gate_val = jnp.dot(rows, weight_gate, preferred_element_type=jnp.float32)
    up_val = jnp.dot(rows, weight_up, preferred_element_type=jnp.float32)
    return (jax.nn.silu(gate_val) * up_val).astype(jnp.bfloat16)


F32 = jnp.float32
BF16 = jnp.bfloat16


def fused_kernel(
    conv_x, conv_c, conv_b, taps, w_out, tokens, gain, coef, w_gate, w_up, w_down,
    mixed_ref, experts_ref,
    full_g, full_u, full_d, full_o, tok, normed, cf, hidden, contrib,
    in_l, in_r, out_l, out_r, cx, cc, cb, hx, hc, ext, gated,
    x_s, x_r, y_s, y_r, dx_s, dx_r, dy_s, dy_r, own_s, own_r,
    zr_s, zr_r, zl_s, zl_r, cf_s, cf_r, h_s, h_r, rl_s, rl_r, rr_s, rr_r, loc,
):
    n_ep, rows, width = tok.shape
    half = rows // 2
    rows_mix = cx.shape[0]
    edge = hx.shape[0]
    last_z = n_ep - 1
    y = lax.axis_index("grp")
    z = lax.axis_index("ep")
    k = lax.axis_index("tp")
    n_tp = full_g.shape[0]
    core = lax.rem(k, 2)
    mate = k + 1 - 2 * core
    far = lax.rem(k + 2, n_tp)
    far_mate = lax.rem(mate + 2, n_tp)
    other_y = 1 - y
    flat = z * n_tp + k
    total = n_ep * n_tp
    nxt = lax.rem(flat + 1, total)
    prv = lax.rem(flat + total - 1, total)
    nxt_id = {"ep": lax.div(nxt, n_tp), "tp": lax.rem(nxt, n_tp)}
    prv_id = {"ep": lax.div(prv, n_tp), "tp": lax.rem(prv, n_tp)}

    def rc(src, dst, send, recv, dev):
        return pltpu.make_async_remote_copy(
            src_ref=src, dst_ref=dst, send_sem=send, recv_sem=recv,
            device_id=dev, device_id_type=pl.DeviceIdType.MESH,
        )

    locals_ = [
        (tokens, tok.at[z]), (coef, cf.at[z]),
        (conv_x, cx), (conv_c, cc), (conv_b, cb),
        (w_gate.at[0], full_g.at[k]), (w_up.at[0], full_u.at[k]),
        (w_down.at[0], full_d.at[k]), (w_out, full_o.at[k]),
    ]
    local_copies = [pltpu.make_async_copy(a, b, loc.at[i]) for i, (a, b) in enumerate(locals_)]
    for cp in local_copies:
        cp.start()

    barrier = pltpu.get_barrier_semaphore()
    peers = [{"tp": mate}, {"tp": far}, {"grp": other_y}, nxt_id, prv_id]
    peers += [{"ep": lax.rem(z + m, n_ep)} for m in range(1, n_ep)]
    for dev in peers:
        pl.semaphore_signal(barrier, inc=1, device_id=dev, device_id_type=pl.DeviceIdType.MESH)
    pl.semaphore_wait(barrier, len(peers))

    pieces = [(w_gate.at[0], full_g, 2), (w_up.at[0], full_u, 2), (w_down.at[0], full_d, 2), (w_out, full_o, 4)]
    chunks = []
    for own, full, cuts in pieces:
        per_half = full.shape[1] // 2
        size = per_half // cuts
        for j in range(cuts):
            chunks.append((own, full, per_half, size, j))
    n_chunks = len(chunks)

    def span(i, h):
        _, _, per_half, size, j = chunks[i]
        return pl.ds(pl.multiple_of(h * per_half + j * size, size), size)

    def x_copy(i):
        own, full = chunks[i][:2]
        return rc(own.at[span(i, y)], full.at[k, span(i, y)], x_s.at[i], x_r.at[i], {"tp": far})

    def y_copy(i):
        at = chunks[i][1].at[far, span(i, y)]
        return rc(at, at, y_s.at[i], y_r.at[i], {"grp": other_y})

    def dx_copy(i):
        at = chunks[i][1].at[far, span(i, y)]
        return rc(at, at, dx_s.at[i], dx_r.at[i], {"tp": mate})

    def dy_copy(i):
        at = chunks[i][1].at[far, span(i, other_y)]
        return rc(at, at, dy_s.at[i], dy_r.at[i], {"tp": mate})

    def own_copy(i):
        own, full, _ = pieces[i]
        return rc(own, full.at[k], own_s.at[i], own_r.at[i], {"tp": mate})

    def got(i, piece, h, send, recv):
        at = chunks[i][1].at[piece, span(i, h)]
        rc(at, at, send.at[i], recv.at[i], {"tp": mate}).wait_recv()

    rows_of = lambda j: pl.ds((j % 2) * half, half)

    def zr_send(j):
        b = z - j // 2
        src = tokens.at[rows_of(j)] if j < 2 else tok.at[b, rows_of(j)]
        return rc(src, tok.at[b, rows_of(j)], zr_s.at[j], zr_r.at[j], {"ep": z + 1})

    def zl_send(j):
        b = z + j // 2
        src = tokens.at[rows_of(j)] if j < 2 else tok.at[b, rows_of(j)]
        return rc(src, tok.at[b, rows_of(j)], zl_s.at[j], zl_r.at[j], {"ep": z - 1})

    def zr_got(j):
        at = tok.at[z - 1 - j // 2, rows_of(j)]
        rc(at, at, zr_s.at[j], zr_r.at[j], {"ep": z - 1}).wait_recv()

    def zl_got(j):
        at = tok.at[z + 1 + j // 2, rows_of(j)]
        rc(at, at, zl_s.at[j], zl_r.at[j], {"ep": z + 1}).wait_recv()

    def cf_copy(m):
        return rc(coef, cf.at[z], cf_s.at[m - 1], cf_r.at[m - 1], {"ep": lax.rem(z + m, n_ep)})

    tail = pl.ds(rows_mix - edge, edge)

    def halo_copies():
        return (
            rc(conv_x.at[tail], hx, h_s.at[0], h_r.at[0], nxt_id),
            rc(conv_c.at[tail], hc, h_s.at[1], h_r.at[1], nxt_id),
        )

    is_first, is_last = flat == 0, flat == total - 1

    for m in range(1, n_ep):
        cf_copy(m).start()

    @pl.when(jnp.logical_not(is_last))
    def _():
        for cp in halo_copies():
            cp.start()

    for j in range(2):
        pl.when(z < last_z)(lambda j=j: zr_send(j).start())
        pl.when(z > 0)(lambda j=j: zl_send(j).start())
    for i in range(n_chunks):
        x_copy(i).start()
    for i in range(len(pieces)):
        own_copy(i).start()
    for cp in local_copies:
        cp.wait()

    @pl.when(is_first)
    def _():
        hx[...] = jnp.zeros_like(hx)
        hc[...] = jnp.zeros_like(hc)

    @pl.when(jnp.logical_not(is_first))
    def _():
        for cp in halo_copies():
            cp.wait_recv()

    n_taps = taps.shape[0]

    def conv_tile(t, _):
        cols = pl.ds(pl.multiple_of(t * 128, 128), 128)
        ext[pl.ds(0, edge), :] = (hc[:, cols].astype(F32) * hx[:, cols].astype(F32)).astype(BF16).astype(F32)
        ext[pl.ds(edge, rows_mix), :] = (cc[:, cols].astype(F32) * cx[:, cols].astype(F32)).astype(BF16).astype(F32)
        filtered = jnp.zeros((rows_mix, 128), F32)
        for s in range(n_taps):
            filtered = filtered + taps[pl.ds(s, 1), cols] * ext[pl.ds(edge - (n_taps - 1) + s, rows_mix), :]
        gated[:, cols] = (cb[:, cols].astype(F32) * filtered).astype(BF16)
        return 0

    lax.fori_loop(0, cx.shape[1] // 128, conv_tile, 0)

    def norm_block(b):
        def body(r, _):
            at = pl.ds(pl.multiple_of(r * 32, 32), 32)
            v = tok[b, at, :].astype(F32)
            scale = lax.rsqrt(jnp.mean(v * v, axis=-1, keepdims=True) + 1e-06)
            normed[pl.ds(pl.multiple_of(b * rows + r * 32, 32), 32), :] = (v * scale * gain[...]).astype(BF16)
            return 0

        lax.fori_loop(0, rows // 32, body, 0)

    norm_block(z)

    def weight_step(i):
        if i < n_chunks:
            got(i, far, y, x_s, x_r)
            y_copy(i).start()
            dx_copy(i).start()
        if 1 <= i <= n_chunks:
            got(i - 1, far, other_y, y_s, y_r)
            dy_copy(i - 1).start()

    def mate_wait(lo, hi):
        for i in range(lo, hi):
            got(i, far_mate, y, dx_s, dx_r)
            got(i, far_mate, other_y, dy_s, dy_r)

    def own_wait(i):
        at = pieces[i][1].at[mate]
        rc(at, at, own_s.at[i], own_r.at[i], {"tp": mate}).wait_recv()

    steps = 2 * last_z
    for s in range(steps):
        @pl.when(s < 2 * z)
        def _():
            zr_got(s)
            if s + 2 < steps:
                pl.when(z < last_z)(lambda: zr_send(s + 2).start())

        @pl.when(s < 2 * (last_z - z))
        def _():
            zl_got(s)
            if s + 2 < steps:
                pl.when(z > 0)(lambda: zl_send(s + 2).start())

        weight_step(s)
        if s % 2 == 1:
            m = s // 2 + 1
            pl.when(z - m >= 0)(lambda: norm_block(z - m))
            pl.when(z + m <= last_z)(lambda: norm_block(z + m))

    mate_wait(0, 4)
    own_wait(0)
    own_wait(1)

    def hidden_piece(p, _):
        g = jnp.dot(normed[...], full_g[p], preferred_element_type=F32)
        u = jnp.dot(normed[...], full_u[p], preferred_element_type=F32)
        hidden[p] = (jax.nn.silu(g) * u).astype(BF16)
        return 0

    lax.fori_loop(0, n_tp, hidden_piece, 0)
    weight_step(6)
    mate_wait(4, 6)
    own_wait(2)
    for m in range(1, n_ep):
        at = cf.at[lax.rem(z + n_ep - m, n_ep)]
        rc(at, at, cf_s.at[m - 1], cf_r.at[m - 1], {"ep": z}).wait_recv()

    eye = lax.broadcasted_iota(jnp.int32, (rows, rows), 0) == lax.broadcasted_iota(jnp.int32, (rows, rows), 1)
    columns = []
    for b in range(n_ep):
        line = cf[b, pl.ds(z, 1), :]
        columns.append(jnp.sum(jnp.where(eye, jnp.broadcast_to(line, (rows, rows)), 0.0), axis=1, keepdims=True))
    column = jnp.concatenate(columns, axis=0)
    tile = 256

    def down_tile(t, _):
        cols = pl.ds(pl.multiple_of(t * tile, tile), tile)
        acc = jnp.dot(hidden[0], full_d[0, :, cols], preferred_element_type=F32)
        for p in range(1, n_tp):
            acc = acc + jnp.dot(hidden[p], full_d[p, :, cols], preferred_element_type=F32)
        contrib[:, cols] = acc * column
        return 0

    lax.fori_loop(0, width // tile, down_tile, 0)

    def own_rows(d, h):
        return contrib[pl.ds(pl.multiple_of(d * rows + h * half, half), half), :]

    def rl_copy(s):
        return rc(out_l.at[s], in_l.at[s], rl_s.at[s], rl_r.at[s], {"ep": z - 1})

    def rr_copy(s):
        return rc(out_r.at[s], in_r.at[s], rr_s.at[s], rr_r.at[s], {"ep": z + 1})

    def rl_got(s):
        rc(in_l.at[s], in_l.at[s], rl_s.at[s], rl_r.at[s], {"ep": z}).wait_recv()

    def rr_got(s):
        rc(in_r.at[s], in_r.at[s], rr_s.at[s], rr_r.at[s], {"ep": z}).wait_recv()

    def side(s, depth, inbox, outbox, got_fn, copy_fn, dest_fn):
        has_in = depth < last_z

        @pl.when(jnp.logical_and(s >= 0, jnp.logical_and(has_in, s < 2 * (depth + 1))))
        def _():
            got_fn(s)

        @pl.when(jnp.logical_and(s >= 0, s < 2 * depth))
        def _():
            mine = own_rows(dest_fn(lax.div(s, 2)), lax.rem(s, 2))

            @pl.when(has_in)
            def _():
                outbox[s] = (mine + inbox[s].astype(F32)).astype(BF16)

            @pl.when(jnp.logical_not(has_in))
            def _():
                outbox[s] = mine.astype(BF16)

            copy_fn(s).start()

    for t in range(steps + 1):
        if t == steps:
            mate_wait(6, n_chunks)
            own_wait(3)

            def mixed_tile(q, _):
                cols = pl.ds(pl.multiple_of(q * tile, tile), tile)
                part = full_o.shape[1]
                acc = jnp.zeros((rows_mix, tile), F32)
                for p in range(n_tp):
                    acc = acc + jnp.dot(gated[:, p * part : (p + 1) * part], full_o[p, :, cols], preferred_element_type=F32)
                mixed_ref[:, cols] = acc.astype(BF16)
                return 0

            lax.fori_loop(0, width // tile, mixed_tile, 0)
        side(t - (last_z - z), z, in_l, out_l, rl_got, rl_copy, lambda b: b)
        side(t - z, last_z - z, in_r, out_r, rr_got, rr_copy, lambda b: last_z - b)
        if 7 + t <= n_chunks:
            weight_step(7 + t)

    for h in range(2):
        at = pl.ds(h * half, half)
        mine = own_rows(z, h)

        @pl.when(z == 0)
        def _():
            experts_ref[at, :] = (mine + in_l[h].astype(F32)).astype(BF16)

        @pl.when(z == last_z)
        def _():
            experts_ref[at, :] = (mine + in_r[h].astype(F32)).astype(BF16)

        @pl.when(jnp.logical_and(z > 0, z < last_z))
        def _():
            experts_ref[at, :] = (
                mine + in_l[2 * z + h].astype(F32) + in_r[2 * (last_z - z) + h].astype(F32)
            ).astype(BF16)

    for i in range(n_chunks):
        x_copy(i).wait_send()
        y_copy(i).wait_send()
        dx_copy(i).wait_send()
        dy_copy(i).wait_send()
    for i in range(len(pieces)):
        own_copy(i).wait_send()
    for m in range(1, n_ep):
        cf_copy(m).wait_send()

    @pl.when(jnp.logical_not(is_last))
    def _():
        for cp in halo_copies():
            cp.wait_send()

    for j in range(steps):
        pl.when(jnp.logical_and(z < last_z, j < 2 * (z + 1)))(lambda j=j: zr_send(j).wait_send())
        pl.when(jnp.logical_and(z > 0, j < 2 * (last_z - z + 1)))(lambda j=j: zl_send(j).wait_send())
        pl.when(j < 2 * z)(lambda j=j: rl_copy(j).wait_send())
        pl.when(j < 2 * (last_z - z))(lambda j=j: rr_copy(j).wait_send())


def per_device_fused(
    conv_x, conv_c, conv_b, conv_taps, w_out, tokens_b, norm_gain,
    route_b, route_weights, w_gate, w_up, w_down,
):
    n_ep, n_tp = lax.axis_size("ep"), lax.axis_size("tp")
    rows, width = tokens_b.shape
    rows_mix, channels = conv_x.shape
    hid = w_gate.shape[2]
    shares = route_weights / jnp.sum(route_weights, axis=-1, keepdims=True)
    lanes = jnp.arange(-(-n_ep // 8) * 8, dtype=jnp.int32)[:, None, None]
    coef = jnp.sum(jnp.where(route_b.T[None] == lanes, shares.T[None], 0.0), axis=1)
    edge, half, steps = 16, rows // 2, 2 * (n_ep - 1)
    n_chunks = 10
    dma = pltpu.SemaphoreType.DMA
    hbm, vmem = pl.BlockSpec(memory_space=pl.ANY), pl.BlockSpec(memory_space=pltpu.VMEM)
    return pl.pallas_call(
        fused_kernel,
        out_shape=(
            jax.ShapeDtypeStruct((rows_mix, width), BF16),
            jax.ShapeDtypeStruct((rows, width), BF16),
        ),
        in_specs=[hbm, hbm, hbm, vmem, hbm, hbm, vmem, hbm, hbm, hbm, hbm],
        out_specs=(vmem, vmem),
        scratch_shapes=[
            pltpu.VMEM((n_tp,) + w_gate.shape[1:], BF16),
            pltpu.VMEM((n_tp,) + w_up.shape[1:], BF16),
            pltpu.VMEM((n_tp,) + w_down.shape[1:], BF16),
            pltpu.VMEM((n_tp,) + w_out.shape, BF16),
            pltpu.VMEM((n_ep, rows, width), BF16),
            pltpu.VMEM((n_ep * rows, width), BF16),
            pltpu.VMEM((n_ep,) + coef.shape, F32),
            pltpu.VMEM((n_tp, n_ep * rows, hid), BF16),
            pltpu.VMEM((n_ep * rows, width), F32),
        ]
        + [pltpu.VMEM((steps, half, width), BF16)] * 4
        + [pltpu.VMEM((rows_mix, channels), BF16)] * 3
        + [pltpu.VMEM((edge, channels), BF16)] * 2
        + [pltpu.VMEM((edge + rows_mix, 128), F32), pltpu.VMEM((rows_mix, channels), BF16)]
        + [dma((n_chunks,))] * 8
        + [dma((4,))] * 2
        + [dma((steps,))] * 4
        + [dma((n_ep - 1,))] * 2
        + [dma((2,))] * 2
        + [dma((steps,))] * 4
        + [dma((9,))],
        compiler_params=pltpu.CompilerParams(
            collective_id=0, has_side_effects=True, vmem_limit_bytes=62 * 1024 * 1024
        ),
    )(conv_x, conv_c, conv_b, conv_taps, w_out, tokens_b, norm_gain[None], coef, w_gate, w_up, w_down)


def per_device(
    conv_x,
    conv_c,
    conv_b,
    conv_taps,
    w_out,
    tokens_b,
    norm_gain,
    route_b,
    route_weights,
    w_gate,
    w_up,
    w_down,
):
    rows_mix = conv_x.shape[0]
    reach_rows = conv_taps.shape[0] - 1
    mixed_u = (conv_c.astype(jnp.float32) * conv_x.astype(jnp.float32)).astype(jnp.bfloat16)
    before = shifted(mixed_u[rows_mix - reach_rows :], ("ep", "tp"), 1)
    extended = jnp.concatenate([before, mixed_u], axis=0)
    filtered = jnp.zeros(mixed_u.shape, jnp.float32)
    for shift_tap in range(reach_rows + 1):
        filtered = filtered + conv_taps[shift_tap][None, :] * extended[
            shift_tap : shift_tap + rows_mix
        ].astype(jnp.float32)
    gated_rows = (conv_b.astype(jnp.float32) * filtered).astype(jnp.bfloat16)
    mixed_out = jnp.dot(
        gated_rows,
        lax.all_gather(w_out, "tp", axis=0, tiled=True),
        preferred_element_type=jnp.float32,
    )
    mixed_a = mixed_out.astype(jnp.bfloat16)
    tokens_f = tokens_b.astype(jnp.float32)
    normed = (
        tokens_f
        * lax.rsqrt(jnp.mean(tokens_f * tokens_f, axis=-1, keepdims=True) + 1e-06)
        * norm_gain
    ).astype(jnp.bfloat16)
    experts = lax.axis_size("ep")
    rows_exp = route_b.shape[0]
    capacity = 2 * rows_exp * TOPK // experts
    slot_total = experts * capacity
    targets = slot_targets(route_b, experts, capacity)
    weight_gate = w_gate[0]
    weight_up = w_up[0]
    weight_down = w_down[0]
    padded_rows = jnp.concatenate([normed, jnp.zeros((1, D), jnp.bfloat16)], axis=0)
    outgoing = padded_rows[fill_slots(targets, slot_total, rows_exp)]
    arrived = lax.all_to_all(outgoing, "ep", split_axis=0, concat_axis=0, tiled=True)
    hidden = expert_hidden(
        lax.all_gather(arrived, "tp", axis=0, tiled=True), weight_gate, weight_up
    )
    summed = lax.psum_scatter(
        jnp.dot(hidden, weight_down, preferred_element_type=jnp.float32).astype(jnp.bfloat16),
        "tp",
        scatter_dimension=0,
        tiled=True,
    )
    returned = lax.all_to_all(summed, "ep", split_axis=0, concat_axis=0, tiled=True)
    picked = returned[targets]
    shares = route_weights / jnp.sum(route_weights, axis=-1, keepdims=True)
    experts_b = jnp.sum(picked.astype(jnp.float32) * shares[:, :, None], axis=1).astype(
        jnp.bfloat16
    )
    return (mixed_a, experts_b)


def solution(mesh):
    dense = mesh.shape["ep"] <= 2 * TOPK and mesh.shape["tp"] == 4 and mesh.shape["grp"] == 2
    return jax.shard_map(
        per_device_fused if dense else per_device,
        mesh=mesh,
        in_specs=(
            P(("grp", "ep", "tp"), None),
            P(("grp", "ep", "tp"), None),
            P(("grp", "ep", "tp"), None),
            P(),
            P("tp", None),
            P(("grp", "ep", "tp"), None),
            P(),
            P(("grp", "ep", "tp"), None),
            P(("grp", "ep", "tp"), None),
            P("ep", None, "tp"),
            P("ep", None, "tp"),
            P("ep", "tp", None),
        ),
        out_specs=(P(("grp", "ep", "tp"), None), P(("grp", "ep", "tp"), None)),
        check_vma=False,
    )
```

```python
import functools
import jax
import jax.numpy as jnp
from jax import lax
from jax.experimental import pallas as pl
from jax.experimental.pallas import tpu as pltpu
from jax.sharding import PartitionSpec as P

D = 2048
TOPK = 2


def shifted(x, axis, by):
    size = lax.axis_size(axis)
    pairs = [(i, i + by) for i in range(size) if 0 <= i + by < size]
    return lax.ppermute(x, axis, pairs)


def slot_targets(route, experts, capacity):
    flat = route.reshape(-1)
    onehot = (flat[:, None] == jnp.arange(experts, dtype=jnp.int32)[None, :]).astype(jnp.int32)
    earlier = jnp.cumsum(onehot, axis=0) - onehot
    ranks = jnp.sum(earlier * onehot, axis=1).reshape(route.shape)
    return route * capacity + ranks


def fill_slots(targets, slot_total, filler):
    token_ids = jnp.repeat(jnp.arange(filler, dtype=jnp.int32), targets.shape[1])
    return jnp.full((slot_total,), filler, jnp.int32).at[targets.reshape(-1)].set(token_ids)


def expert_hidden(rows, weight_gate, weight_up):
    gate_val = jnp.dot(rows, weight_gate, preferred_element_type=jnp.float32)
    up_val = jnp.dot(rows, weight_up, preferred_element_type=jnp.float32)
    return (jax.nn.silu(gate_val) * up_val).astype(jnp.bfloat16)


F32 = jnp.float32
BF16 = jnp.bfloat16
CUTS = ((2, (1,)), (2, (1,)), (1, (2, 1)), (4, (1,)))


def fused_kernel(
    conv_x, conv_c, conv_b, taps, w_out, tokens, gain, route, weights, w_gate, w_up, w_down,
    mixed_ref, experts_ref,
    full_g, full_u, full_d, full_o, tok, normed, rt, wt, hidden, contrib,
    in_l, in_r, out_l, out_r, cx, cc, cb, hx, hc, ext, gated,
    x_s, x_r, y_s, y_r, dx_s, dx_r, dy_s, dy_r, own_s, own_r,
    zr_s, zr_r, zl_s, zl_r, rt_s, rt_r, wt_s, wt_r, h_s, h_r, rl_s, rl_r, rr_s, rr_r, loc,
):
    n_ep, rows, width = tok.shape
    half = rows // 2
    rows_mix = cx.shape[0]
    edge = hx.shape[0]
    last_z = n_ep - 1
    y = lax.axis_index("grp")
    z = lax.axis_index("ep")
    k = lax.axis_index("tp")
    n_tp = full_g.shape[0]
    core = lax.rem(k, 2)
    mate = k + 1 - 2 * core
    far = lax.rem(k + 2, n_tp)
    far_mate = lax.rem(mate + 2, n_tp)
    other_y = 1 - y
    flat = z * n_tp + k
    total = n_ep * n_tp
    nxt = lax.rem(flat + 1, total)
    prv = lax.rem(flat + total - 1, total)
    nxt_id = {"ep": lax.div(nxt, n_tp), "tp": lax.rem(nxt, n_tp)}
    prv_id = {"ep": lax.div(prv, n_tp), "tp": lax.rem(prv, n_tp)}

    def rc(src, dst, send, recv, dev):
        return pltpu.make_async_remote_copy(
            src_ref=src, dst_ref=dst, send_sem=send, recv_sem=recv,
            device_id=dev, device_id_type=pl.DeviceIdType.MESH,
        )

    locals_ = [
        (tokens, tok.at[z]), (route, rt.at[z]), (weights, wt.at[z]),
        (conv_x, cx), (conv_c, cc), (conv_b, cb),
        (w_gate.at[0], full_g.at[k]), (w_up.at[0], full_u.at[k]),
        (w_down.at[0], full_d.at[k]), (w_out, full_o.at[k]),
    ]
    local_copies = [pltpu.make_async_copy(a, b, loc.at[i]) for i, (a, b) in enumerate(locals_)]
    for cp in local_copies:
        cp.start()

    barrier = pltpu.get_barrier_semaphore()
    peers = [{"tp": mate}, {"tp": far}, {"grp": other_y}, nxt_id, prv_id]
    peers += [{"ep": lax.rem(z + m, n_ep)} for m in range(1, n_ep)]
    for dev in peers:
        pl.semaphore_signal(barrier, inc=1, device_id=dev, device_id_type=pl.DeviceIdType.MESH)
    pl.semaphore_wait(barrier, len(peers))

    pieces = [(w_gate.at[0], full_g), (w_up.at[0], full_u), (w_down.at[0], full_d), (w_out, full_o)]
    out_cols = full_d.shape[2] // 2
    chunks = []
    for at, (rows_cut, cols_cut) in enumerate(CUTS):
        half_rows, cols = pieces[at][1].shape[1] // 2, pieces[at][1].shape[2]
        for c, cuts in enumerate(cols_cut):
            for j in range(rows_cut * cuts):
                size = half_rows // (rows_cut * cuts)
                wide = cols // len(cols_cut)
                chunks.append((at, j * size, size, c * wide, wide))
    n_chunks = len(chunks)

    def part(i, ref, h):
        at, first, size, col, wide = chunks[i]
        start = pl.multiple_of(h * (pieces[at][1].shape[1] // 2) + first, size)
        return ref.at[pl.ds(start, size), pl.ds(col, wide)]

    def full_at(i, piece, h):
        return part(i, pieces[chunks[i][0]][1].at[piece], h)

    def x_copy(i):
        return rc(part(i, pieces[chunks[i][0]][0], y), full_at(i, k, y), x_s.at[i], x_r.at[i], {"tp": far})

    def y_copy(i):
        at = full_at(i, far, y)
        return rc(at, at, y_s.at[i], y_r.at[i], {"grp": other_y})

    def dx_copy(i):
        at = full_at(i, far, y)
        return rc(at, at, dx_s.at[i], dx_r.at[i], {"tp": mate})

    def dy_copy(i):
        at = full_at(i, far, other_y)
        return rc(at, at, dy_s.at[i], dy_r.at[i], {"tp": mate})

    def own_copy(i):
        own, full = pieces[i]
        return rc(own, full.at[k], own_s.at[i], own_r.at[i], {"tp": mate})

    def got(i, piece, h, send, recv):
        at = full_at(i, piece, h)
        rc(at, at, send.at[i], recv.at[i], {"tp": mate}).wait_recv()

    rows_of = lambda j: pl.ds((j % 2) * half, half)

    def zr_send(j):
        b = z - j // 2
        src = tokens.at[rows_of(j)] if j < 2 else tok.at[b, rows_of(j)]
        return rc(src, tok.at[b, rows_of(j)], zr_s.at[j], zr_r.at[j], {"ep": z + 1})

    def zl_send(j):
        b = z + j // 2
        src = tokens.at[rows_of(j)] if j < 2 else tok.at[b, rows_of(j)]
        return rc(src, tok.at[b, rows_of(j)], zl_s.at[j], zl_r.at[j], {"ep": z - 1})

    def zr_got(j):
        at = tok.at[z - 1 - j // 2, rows_of(j)]
        rc(at, at, zr_s.at[j], zr_r.at[j], {"ep": z - 1}).wait_recv()

    def zl_got(j):
        at = tok.at[z + 1 + j // 2, rows_of(j)]
        rc(at, at, zl_s.at[j], zl_r.at[j], {"ep": z + 1}).wait_recv()

    def route_copies(m, here, there):
        dev = {"ep": there}
        return (
            rc(route, rt.at[here], rt_s.at[m - 1], rt_r.at[m - 1], dev),
            rc(weights, wt.at[here], wt_s.at[m - 1], wt_r.at[m - 1], dev),
        )

    def routes_out(m):
        return route_copies(m, z, lax.rem(z + m, n_ep))

    tail = pl.ds(rows_mix - edge, edge)

    def halo_copies():
        return (
            rc(conv_x.at[tail], hx, h_s.at[0], h_r.at[0], nxt_id),
            rc(conv_c.at[tail], hc, h_s.at[1], h_r.at[1], nxt_id),
        )

    is_first, is_last = flat == 0, flat == total - 1

    for m in range(1, n_ep):
        for cp in routes_out(m):
            cp.start()

    @pl.when(jnp.logical_not(is_last))
    def _():
        for cp in halo_copies():
            cp.start()

    for j in range(2):
        pl.when(z < last_z)(lambda j=j: zr_send(j).start())
        pl.when(z > 0)(lambda j=j: zl_send(j).start())
    for i in range(n_chunks):
        x_copy(i).start()
    for i in range(len(pieces)):
        own_copy(i).start()
    for cp in local_copies:
        cp.wait()

    @pl.when(is_first)
    def _():
        hx[...] = jnp.zeros_like(hx)
        hc[...] = jnp.zeros_like(hc)

    @pl.when(jnp.logical_not(is_first))
    def _():
        for cp in halo_copies():
            cp.wait_recv()

    n_taps = taps.shape[0]

    def conv_tile(t, _):
        cols = pl.ds(pl.multiple_of(t * 128, 128), 128)
        ext[pl.ds(0, edge), :] = (hc[:, cols].astype(F32) * hx[:, cols].astype(F32)).astype(BF16).astype(F32)
        ext[pl.ds(edge, rows_mix), :] = (cc[:, cols].astype(F32) * cx[:, cols].astype(F32)).astype(BF16).astype(F32)
        filtered = jnp.zeros((rows_mix, 128), F32)
        for s in range(n_taps):
            filtered = filtered + taps[pl.ds(s, 1), cols] * ext[pl.ds(edge - (n_taps - 1) + s, rows_mix), :]
        gated[:, cols] = (cb[:, cols].astype(F32) * filtered).astype(BF16)
        return 0

    lax.fori_loop(0, cx.shape[1] // 128, conv_tile, 0)

    def norm_block(b):
        def body(r, _):
            at = pl.ds(pl.multiple_of(r * 32, 32), 32)
            v = tok[b, at, :].astype(F32)
            scale = lax.rsqrt(jnp.mean(v * v, axis=-1, keepdims=True) + 1e-06)
            normed[pl.ds(pl.multiple_of(b * rows + r * 32, 32), 32), :] = (v * scale * gain[...]).astype(BF16)
            return 0

        lax.fori_loop(0, rows // 32, body, 0)

    first_near = k - core
    first_far = n_tp - 2 - first_near

    def hidden_of(p, at):
        g = jnp.dot(normed[at, :], full_g[p], preferred_element_type=F32)
        u = jnp.dot(normed[at, :], full_u[p], preferred_element_type=F32)
        hidden[p, at, :] = (jax.nn.silu(g) * u).astype(BF16)

    def near_block(b):
        norm_block(b)
        at = pl.ds(pl.multiple_of(b * rows, rows), rows)

        def body(m, _):
            hidden_of(first_near + m, at)
            return 0

        lax.fori_loop(0, 2, body, 0)

    def weight_step(i, with_y=True, with_x=True):
        if with_x and i < n_chunks:
            got(i, far, y, x_s, x_r)
            y_copy(i).start()
            dx_copy(i).start()
        if with_y and 1 <= i <= n_chunks:
            got(i - 1, far, other_y, y_s, y_r)
            dy_copy(i - 1).start()

    def mate_wait(lo, hi):
        for i in range(lo, hi):
            got(i, far_mate, y, dx_s, dx_r)
            got(i, far_mate, other_y, dy_s, dy_r)

    def own_wait(i):
        at = pieces[i][1].at[mate]
        rc(at, at, own_s.at[i], own_r.at[i], {"tp": mate}).wait_recv()

    own_wait(0)
    own_wait(1)
    near_block(z)

    steps = 2 * last_z
    for s in range(steps):
        @pl.when(s < 2 * z)
        def _():
            zr_got(s)
            if s + 2 < steps:
                pl.when(z < last_z)(lambda: zr_send(s + 2).start())

        @pl.when(s < 2 * (last_z - z))
        def _():
            zl_got(s)
            if s + 2 < steps:
                pl.when(z > 0)(lambda: zl_send(s + 2).start())

        weight_step(s)
        if s % 2 == 1:
            m = s // 2 + 1
            pl.when(z - m >= 0)(lambda: near_block(z - m))
            pl.when(z + m <= last_z)(lambda: near_block(z + m))

    mate_wait(0, 4)

    def far_piece(m, _):
        hidden_of(first_far + m, pl.ds(0, n_ep * rows))
        return 0

    lax.fori_loop(0, 2, far_piece, 0)
    weight_step(6, with_x=False)
    weight_step(6, with_y=False)
    mate_wait(4, 6)
    own_wait(2)
    for m in range(1, n_ep):
        for cp in route_copies(m, lax.rem(z + n_ep - m, n_ep), z):
            cp.wait_recv()

    eye = lax.broadcasted_iota(jnp.int32, (rows, rows), 0) == lax.broadcasted_iota(jnp.int32, (rows, rows), 1)
    columns = []
    for b in range(n_ep):
        w = wt[b]
        share = w / jnp.sum(w, axis=0, keepdims=True)
        line = jnp.sum(jnp.where(rt[b] == z, share, 0.0), axis=0, keepdims=True)
        columns.append(jnp.sum(jnp.where(eye, jnp.broadcast_to(line, (rows, rows)), 0.0), axis=1, keepdims=True))
    column = jnp.concatenate(columns, axis=0)
    tile = 256

    def down_half(c):
        def body(t, _):
            cols = pl.ds(pl.multiple_of(c * out_cols + t * tile, tile), tile)
            acc = jnp.dot(hidden[0], full_d[0, :, cols], preferred_element_type=F32)
            for p in range(1, n_tp):
                acc = acc + jnp.dot(hidden[p], full_d[p, :, cols], preferred_element_type=F32)
            contrib[:, cols] = acc * column
            return 0

        lax.fori_loop(0, out_cols // tile, body, 0)

    down_half(0)

    def own_part(d, c):
        return contrib[
            pl.ds(pl.multiple_of(d * rows, rows), rows), pl.ds(pl.multiple_of(c * out_cols, out_cols), out_cols)
        ]

    def rl_copy(s):
        return rc(out_l.at[s], in_l.at[s], rl_s.at[s], rl_r.at[s], {"ep": z - 1})

    def rr_copy(s):
        return rc(out_r.at[s], in_r.at[s], rr_s.at[s], rr_r.at[s], {"ep": z + 1})

    def rl_got(s):
        rc(in_l.at[s], in_l.at[s], rl_s.at[s], rl_r.at[s], {"ep": z}).wait_recv()

    def rr_got(s):
        rc(in_r.at[s], in_r.at[s], rr_s.at[s], rr_r.at[s], {"ep": z}).wait_recv()

    def side(s, depth, inbox, outbox, got_fn, copy_fn, dest_fn):
        has_in = depth < last_z

        c, d = lax.div(s, last_z), lax.rem(s, last_z)
        live = jnp.logical_and(s >= 0, s < steps)

        @pl.when(jnp.logical_and(live, jnp.logical_and(has_in, d <= depth)))
        def _():
            got_fn(s)

        @pl.when(jnp.logical_and(live, d < depth))
        def _():
            mine = own_part(dest_fn(d), c)

            @pl.when(has_in)
            def _():
                outbox[s] = (mine + inbox[s].astype(F32)).astype(BF16)

            @pl.when(jnp.logical_not(has_in))
            def _():
                outbox[s] = mine.astype(BF16)

            copy_fn(s).start()

    def mixed_tile(q, _):
        cols = pl.ds(pl.multiple_of(q * tile, tile), tile)
        block = full_o.shape[1]
        acc = jnp.zeros((rows_mix, tile), F32)
        for p in range(n_tp):
            acc = acc + jnp.dot(gated[:, p * block : (p + 1) * block], full_o[p, :, cols], preferred_element_type=F32)
        mixed_ref[:, cols] = acc.astype(BF16)
        return 0

    for t in range(steps + last_z - 1):
        if t == 2:
            mate_wait(6, 7)
            down_half(1)
        if t == steps:
            mate_wait(7, n_chunks)
            own_wait(3)
            lax.fori_loop(0, width // tile, mixed_tile, 0)
        side(t - (last_z - z), z, in_l, out_l, rl_got, rl_copy, lambda b: b)
        side(t - z, last_z - z, in_r, out_r, rr_got, rr_copy, lambda b: last_z - b)
        if 7 + t <= n_chunks:
            weight_step(7 + t)

    for c in range(2):
        cols = pl.ds(c * out_cols, out_cols)
        mine = own_part(z, c)

        @pl.when(z == 0)
        def _():
            experts_ref[:, cols] = (mine + in_l[c * last_z].astype(F32)).astype(BF16)

        @pl.when(z == last_z)
        def _():
            experts_ref[:, cols] = (mine + in_r[c * last_z].astype(F32)).astype(BF16)

        @pl.when(jnp.logical_and(z > 0, z < last_z))
        def _():
            experts_ref[:, cols] = (
                mine + in_l[c * last_z + z].astype(F32) + in_r[c * last_z + last_z - z].astype(F32)
            ).astype(BF16)

    for i in range(n_chunks):
        x_copy(i).wait_send()
        y_copy(i).wait_send()
        dx_copy(i).wait_send()
        dy_copy(i).wait_send()
    for i in range(len(pieces)):
        own_copy(i).wait_send()
    for m in range(1, n_ep):
        for cp in routes_out(m):
            cp.wait_send()

    @pl.when(jnp.logical_not(is_last))
    def _():
        for cp in halo_copies():
            cp.wait_send()

    for j in range(steps):
        pl.when(jnp.logical_and(z < last_z, j < 2 * (z + 1)))(lambda j=j: zr_send(j).wait_send())
        pl.when(jnp.logical_and(z > 0, j < 2 * (last_z - z + 1)))(lambda j=j: zl_send(j).wait_send())
        pl.when(j % last_z < z)(lambda j=j: rl_copy(j).wait_send())
        pl.when(j % last_z < last_z - z)(lambda j=j: rr_copy(j).wait_send())


def per_device_fused(
    conv_x, conv_c, conv_b, conv_taps, w_out, tokens_b, norm_gain,
    route_b, route_weights, w_gate, w_up, w_down,
):
    n_ep, n_tp = lax.axis_size("ep"), lax.axis_size("tp")
    rows, width = tokens_b.shape
    rows_mix, channels = conv_x.shape
    hid = w_gate.shape[2]
    edge, half, steps = 16, rows // 2, 2 * (n_ep - 1)
    n_chunks = sum(n * sum(cols) for n, cols in CUTS)
    dma = pltpu.SemaphoreType.DMA
    hbm, vmem = pl.BlockSpec(memory_space=pl.ANY), pl.BlockSpec(memory_space=pltpu.VMEM)
    return pl.pallas_call(
        fused_kernel,
        out_shape=(
            jax.ShapeDtypeStruct((rows_mix, width), BF16),
            jax.ShapeDtypeStruct((rows, width), BF16),
        ),
        in_specs=[hbm, hbm, hbm, vmem, hbm, hbm, vmem, hbm, hbm, hbm, hbm, hbm],
        out_specs=(vmem, vmem),
        scratch_shapes=[
            pltpu.VMEM((n_tp,) + w_gate.shape[1:], BF16),
            pltpu.VMEM((n_tp,) + w_up.shape[1:], BF16),
            pltpu.VMEM((n_tp,) + w_down.shape[1:], BF16),
            pltpu.VMEM((n_tp,) + w_out.shape, BF16),
            pltpu.VMEM((n_ep, rows, width), BF16),
            pltpu.VMEM((n_ep * rows, width), BF16),
            pltpu.VMEM((n_ep, TOPK, rows), jnp.int32),
            pltpu.VMEM((n_ep, TOPK, rows), F32),
            pltpu.VMEM((n_tp, n_ep * rows, hid), BF16),
            pltpu.VMEM((n_ep * rows, width), F32),
        ]
        + [pltpu.VMEM((steps, rows, width // 2), BF16)] * 4
        + [pltpu.VMEM((rows_mix, channels), BF16)] * 3
        + [pltpu.VMEM((edge, channels), BF16)] * 2
        + [pltpu.VMEM((edge + rows_mix, 128), F32), pltpu.VMEM((rows_mix, channels), BF16)]
        + [dma((n_chunks,))] * 8
        + [dma((4,))] * 2
        + [dma((steps,))] * 4
        + [dma((n_ep - 1,))] * 4
        + [dma((2,))] * 2
        + [dma((steps,))] * 4
        + [dma((10,))],
        compiler_params=pltpu.CompilerParams(
            collective_id=0, has_side_effects=True, vmem_limit_bytes=62 * 1024 * 1024
        ),
    )(conv_x, conv_c, conv_b, conv_taps, w_out, tokens_b, norm_gain[None], route_b.T, route_weights.T, w_gate, w_up, w_down)


def per_device(
    conv_x,
    conv_c,
    conv_b,
    conv_taps,
    w_out,
    tokens_b,
    norm_gain,
    route_b,
    route_weights,
    w_gate,
    w_up,
    w_down,
):
    rows_mix = conv_x.shape[0]
    reach_rows = conv_taps.shape[0] - 1
    mixed_u = (conv_c.astype(jnp.float32) * conv_x.astype(jnp.float32)).astype(jnp.bfloat16)
    before = shifted(mixed_u[rows_mix - reach_rows :], ("ep", "tp"), 1)
    extended = jnp.concatenate([before, mixed_u], axis=0)
    filtered = jnp.zeros(mixed_u.shape, jnp.float32)
    for shift_tap in range(reach_rows + 1):
        filtered = filtered + conv_taps[shift_tap][None, :] * extended[
            shift_tap : shift_tap + rows_mix
        ].astype(jnp.float32)
    gated_rows = (conv_b.astype(jnp.float32) * filtered).astype(jnp.bfloat16)
    mixed_out = jnp.dot(
        gated_rows,
        lax.all_gather(w_out, "tp", axis=0, tiled=True),
        preferred_element_type=jnp.float32,
    )
    mixed_a = mixed_out.astype(jnp.bfloat16)
    tokens_f = tokens_b.astype(jnp.float32)
    normed = (
        tokens_f
        * lax.rsqrt(jnp.mean(tokens_f * tokens_f, axis=-1, keepdims=True) + 1e-06)
        * norm_gain
    ).astype(jnp.bfloat16)
    experts = lax.axis_size("ep")
    rows_exp = route_b.shape[0]
    capacity = 2 * rows_exp * TOPK // experts
    slot_total = experts * capacity
    targets = slot_targets(route_b, experts, capacity)
    weight_gate = w_gate[0]
    weight_up = w_up[0]
    weight_down = w_down[0]
    padded_rows = jnp.concatenate([normed, jnp.zeros((1, D), jnp.bfloat16)], axis=0)
    outgoing = padded_rows[fill_slots(targets, slot_total, rows_exp)]
    arrived = lax.all_to_all(outgoing, "ep", split_axis=0, concat_axis=0, tiled=True)
    hidden = expert_hidden(
        lax.all_gather(arrived, "tp", axis=0, tiled=True), weight_gate, weight_up
    )
    summed = lax.psum_scatter(
        jnp.dot(hidden, weight_down, preferred_element_type=jnp.float32).astype(jnp.bfloat16),
        "tp",
        scatter_dimension=0,
        tiled=True,
    )
    returned = lax.all_to_all(summed, "ep", split_axis=0, concat_axis=0, tiled=True)
    picked = returned[targets]
    shares = route_weights / jnp.sum(route_weights, axis=-1, keepdims=True)
    experts_b = jnp.sum(picked.astype(jnp.float32) * shares[:, :, None], axis=1).astype(
        jnp.bfloat16
    )
    return (mixed_a, experts_b)


def solution(mesh):
    dense = mesh.shape["ep"] <= 2 * TOPK and mesh.shape["tp"] == 4 and mesh.shape["grp"] == 2
    return jax.shard_map(
        per_device_fused if dense else per_device,
        mesh=mesh,
        in_specs=(
            P(("grp", "ep", "tp"), None),
            P(("grp", "ep", "tp"), None),
            P(("grp", "ep", "tp"), None),
            P(),
            P("tp", None),
            P(("grp", "ep", "tp"), None),
            P(),
            P(("grp", "ep", "tp"), None),
            P(("grp", "ep", "tp"), None),
            P("ep", None, "tp"),
            P("ep", None, "tp"),
            P("ep", "tp", None),
        ),
        out_specs=(P(("grp", "ep", "tp"), None), P(("grp", "ep", "tp"), None)),
        check_vma=False,
    )
```

```python
import functools
import jax
import jax.numpy as jnp
from jax import lax
from jax.experimental import pallas as pl
from jax.experimental.pallas import tpu as pltpu
from jax.sharding import PartitionSpec as P

D = 2048
TOPK = 2


def shifted(x, axis, by):
    size = lax.axis_size(axis)
    pairs = [(i, i + by) for i in range(size) if 0 <= i + by < size]
    return lax.ppermute(x, axis, pairs)


def slot_targets(route, experts, capacity):
    flat = route.reshape(-1)
    onehot = (flat[:, None] == jnp.arange(experts, dtype=jnp.int32)[None, :]).astype(jnp.int32)
    earlier = jnp.cumsum(onehot, axis=0) - onehot
    ranks = jnp.sum(earlier * onehot, axis=1).reshape(route.shape)
    return route * capacity + ranks


def fill_slots(targets, slot_total, filler):
    token_ids = jnp.repeat(jnp.arange(filler, dtype=jnp.int32), targets.shape[1])
    return jnp.full((slot_total,), filler, jnp.int32).at[targets.reshape(-1)].set(token_ids)


def expert_hidden(rows, weight_gate, weight_up):
    gate_val = jnp.dot(rows, weight_gate, preferred_element_type=jnp.float32)
    up_val = jnp.dot(rows, weight_up, preferred_element_type=jnp.float32)
    return (jax.nn.silu(gate_val) * up_val).astype(jnp.bfloat16)


F32 = jnp.float32
BF16 = jnp.bfloat16
CUTS = ((2, (1,)), (2, (1,)), (1, (2, 1)), (4, (1,)))


def fused_kernel(
    conv_x, conv_c, conv_b, taps, w_out, tokens, gain, route, weights, w_gate, w_up, w_down,
    mixed_ref, experts_ref,
    full_g, full_u, full_d, full_o, tok, normed, rt, wt, hidden, contrib,
    in_l, in_r, out_l, out_r, cx, cc, cb, hx, hc, ext, gated,
    x_s, x_r, y_s, y_r, dx_s, dx_r, dy_s, dy_r, own_s, own_r,
    zr_s, zr_r, zl_s, zl_r, rt_s, rt_r, wt_s, wt_r, h_s, h_r, rl_s, rl_r, rr_s, rr_r, loc,
):
    n_ep, rows, width = tok.shape
    half = rows // 2
    rows_mix = cx.shape[0]
    edge = hx.shape[0]
    last_z = n_ep - 1
    y = lax.axis_index("grp")
    z = lax.axis_index("ep")
    k = lax.axis_index("tp")
    n_tp = full_g.shape[0]
    core = lax.rem(k, 2)
    mate = k + 1 - 2 * core
    far = lax.rem(k + 2, n_tp)
    far_mate = lax.rem(mate + 2, n_tp)
    other_y = 1 - y
    flat = z * n_tp + k
    total = n_ep * n_tp
    nxt = lax.rem(flat + 1, total)
    prv = lax.rem(flat + total - 1, total)
    nxt_id = {"ep": lax.div(nxt, n_tp), "tp": lax.rem(nxt, n_tp)}
    prv_id = {"ep": lax.div(prv, n_tp), "tp": lax.rem(prv, n_tp)}

    def rc(src, dst, send, recv, dev):
        return pltpu.make_async_remote_copy(
            src_ref=src, dst_ref=dst, send_sem=send, recv_sem=recv,
            device_id=dev, device_id_type=pl.DeviceIdType.MESH,
        )

    locals_ = [
        (tokens, tok.at[z]), (route, rt.at[z]), (weights, wt.at[z]),
        (conv_x, cx), (conv_c, cc), (conv_b, cb),
        (w_gate.at[0], full_g.at[k]), (w_up.at[0], full_u.at[k]),
        (w_down.at[0], full_d.at[k]), (w_out, full_o.at[k]),
    ]
    local_copies = [pltpu.make_async_copy(a, b, loc.at[i]) for i, (a, b) in enumerate(locals_)]
    for cp in local_copies:
        cp.start()

    barrier = pltpu.get_barrier_semaphore()
    peers = [{"tp": mate}, {"tp": far}, {"grp": other_y}, nxt_id, prv_id]
    peers += [{"ep": lax.rem(z + m, n_ep)} for m in range(1, n_ep)]
    for dev in peers:
        pl.semaphore_signal(barrier, inc=1, device_id=dev, device_id_type=pl.DeviceIdType.MESH)
    pl.semaphore_wait(barrier, len(peers))

    pieces = [(w_gate.at[0], full_g), (w_up.at[0], full_u), (w_down.at[0], full_d), (w_out, full_o)]
    out_cols = full_d.shape[2] // 2
    chunks = []
    for at, (rows_cut, cols_cut) in enumerate(CUTS):
        half_rows, cols = pieces[at][1].shape[1] // 2, pieces[at][1].shape[2]
        for c, cuts in enumerate(cols_cut):
            for j in range(rows_cut * cuts):
                size = half_rows // (rows_cut * cuts)
                wide = cols // len(cols_cut)
                chunks.append((at, j * size, size, c * wide, wide))
    n_chunks = len(chunks)

    def part(i, ref, h):
        at, first, size, col, wide = chunks[i]
        start = pl.multiple_of(h * (pieces[at][1].shape[1] // 2) + first, size)
        return ref.at[pl.ds(start, size), pl.ds(col, wide)]

    def full_at(i, piece, h):
        return part(i, pieces[chunks[i][0]][1].at[piece], h)

    def x_copy(i):
        return rc(part(i, pieces[chunks[i][0]][0], y), full_at(i, k, y), x_s.at[i], x_r.at[i], {"tp": far})

    def y_copy(i):
        at = full_at(i, far, y)
        return rc(at, at, y_s.at[i], y_r.at[i], {"grp": other_y})

    def dx_copy(i):
        at = full_at(i, far, y)
        return rc(at, at, dx_s.at[i], dx_r.at[i], {"tp": mate})

    def dy_copy(i):
        at = full_at(i, far, other_y)
        return rc(at, at, dy_s.at[i], dy_r.at[i], {"tp": mate})

    def own_copy(i):
        own, full = pieces[i]
        return rc(own, full.at[k], own_s.at[i], own_r.at[i], {"tp": mate})

    def got(i, piece, h, send, recv):
        at = full_at(i, piece, h)
        rc(at, at, send.at[i], recv.at[i], {"tp": mate}).wait_recv()

    rows_of = lambda j: pl.ds((j % 2) * half, half)

    def zr_send(j):
        b = z - j // 2
        src = tokens.at[rows_of(j)] if j < 2 else tok.at[b, rows_of(j)]
        return rc(src, tok.at[b, rows_of(j)], zr_s.at[j], zr_r.at[j], {"ep": z + 1})

    def zl_send(j):
        b = z + j // 2
        src = tokens.at[rows_of(j)] if j < 2 else tok.at[b, rows_of(j)]
        return rc(src, tok.at[b, rows_of(j)], zl_s.at[j], zl_r.at[j], {"ep": z - 1})

    def zr_got(j):
        at = tok.at[z - 1 - j // 2, rows_of(j)]
        rc(at, at, zr_s.at[j], zr_r.at[j], {"ep": z - 1}).wait_recv()

    def zl_got(j):
        at = tok.at[z + 1 + j // 2, rows_of(j)]
        rc(at, at, zl_s.at[j], zl_r.at[j], {"ep": z + 1}).wait_recv()

    def route_copies(m, here, there):
        dev = {"ep": there}
        return (
            rc(route, rt.at[here], rt_s.at[m - 1], rt_r.at[m - 1], dev),
            rc(weights, wt.at[here], wt_s.at[m - 1], wt_r.at[m - 1], dev),
        )

    def routes_out(m):
        return route_copies(m, z, lax.rem(z + m, n_ep))

    tail = pl.ds(rows_mix - edge, edge)

    def halo_copies():
        return (
            rc(conv_x.at[tail], hx, h_s.at[0], h_r.at[0], nxt_id),
            rc(conv_c.at[tail], hc, h_s.at[1], h_r.at[1], nxt_id),
        )

    is_first, is_last = flat == 0, flat == total - 1

    for m in range(1, n_ep):
        for cp in routes_out(m):
            cp.start()

    @pl.when(jnp.logical_not(is_last))
    def _():
        for cp in halo_copies():
            cp.start()

    for j in range(2):
        pl.when(z < last_z)(lambda j=j: zr_send(j).start())
        pl.when(z > 0)(lambda j=j: zl_send(j).start())
    for i in range(n_chunks):
        x_copy(i).start()
    for i in range(len(pieces)):
        own_copy(i).start()
    for cp in local_copies:
        cp.wait()

    @pl.when(is_first)
    def _():
        hx[...] = jnp.zeros_like(hx)
        hc[...] = jnp.zeros_like(hc)

    @pl.when(jnp.logical_not(is_first))
    def _():
        for cp in halo_copies():
            cp.wait_recv()

    n_taps = taps.shape[0]

    def conv_tile(t, _):
        cols = pl.ds(pl.multiple_of(t * 128, 128), 128)
        ext[pl.ds(0, edge), :] = (hc[:, cols].astype(F32) * hx[:, cols].astype(F32)).astype(BF16).astype(F32)
        ext[pl.ds(edge, rows_mix), :] = (cc[:, cols].astype(F32) * cx[:, cols].astype(F32)).astype(BF16).astype(F32)
        filtered = jnp.zeros((rows_mix, 128), F32)
        for s in range(n_taps):
            filtered = filtered + taps[pl.ds(s, 1), cols] * ext[pl.ds(edge - (n_taps - 1) + s, rows_mix), :]
        gated[:, cols] = (cb[:, cols].astype(F32) * filtered).astype(BF16)
        return 0

    lax.fori_loop(0, cx.shape[1] // 128, conv_tile, 0)

    def norm_block(b):
        def body(r, _):
            at = pl.ds(pl.multiple_of(r * 32, 32), 32)
            v = tok[b, at, :].astype(F32)
            scale = lax.rsqrt(jnp.mean(v * v, axis=-1, keepdims=True) + 1e-06)
            normed[pl.ds(pl.multiple_of(b * rows + r * 32, 32), 32), :] = (v * scale * gain[...]).astype(BF16)
            return 0

        lax.fori_loop(0, rows // 32, body, 0)

    first_near = k - core
    first_far = n_tp - 2 - first_near

    def hidden_of(p, at):
        g = jnp.dot(normed[at, :], full_g[p], preferred_element_type=F32)
        u = jnp.dot(normed[at, :], full_u[p], preferred_element_type=F32)
        hidden[p, at, :] = (jax.nn.silu(g) * u).astype(BF16)

    def near_block(b):
        norm_block(b)
        at = pl.ds(pl.multiple_of(b * rows, rows), rows)

        def body(m, _):
            hidden_of(first_near + m, at)
            return 0

        lax.fori_loop(0, 2, body, 0)

    def weight_step(i, with_y=True, with_x=True):
        if with_x and i < n_chunks:
            got(i, far, y, x_s, x_r)
            y_copy(i).start()
            dx_copy(i).start()
        if with_y and 1 <= i <= n_chunks:
            got(i - 1, far, other_y, y_s, y_r)
            dy_copy(i - 1).start()

    def mate_wait(lo, hi):
        for i in range(lo, hi):
            got(i, far_mate, y, dx_s, dx_r)
            got(i, far_mate, other_y, dy_s, dy_r)

    def own_wait(i):
        at = pieces[i][1].at[mate]
        rc(at, at, own_s.at[i], own_r.at[i], {"tp": mate}).wait_recv()

    own_wait(0)
    own_wait(1)
    near_block(z)

    steps = 2 * last_z
    for s in range(steps):
        @pl.when(s < 2 * z)
        def _():
            zr_got(s)
            if s + 2 < steps:
                pl.when(z < last_z)(lambda: zr_send(s + 2).start())

        @pl.when(s < 2 * (last_z - z))
        def _():
            zl_got(s)
            if s + 2 < steps:
                pl.when(z > 0)(lambda: zl_send(s + 2).start())

        weight_step(s)
        if s % 2 == 1:
            m = s // 2 + 1
            pl.when(z - m >= 0)(lambda: near_block(z - m))
            pl.when(z + m <= last_z)(lambda: near_block(z + m))

    mate_wait(0, 4)

    def far_piece(m, _):
        hidden_of(first_far + m, pl.ds(0, n_ep * rows))
        return 0

    lax.fori_loop(0, 2, far_piece, 0)
    weight_step(6, with_x=False)
    weight_step(6, with_y=False)
    mate_wait(4, 6)
    own_wait(2)
    for m in range(1, n_ep):
        for cp in route_copies(m, lax.rem(z + n_ep - m, n_ep), z):
            cp.wait_recv()

    eye = lax.broadcasted_iota(jnp.int32, (rows, rows), 0) == lax.broadcasted_iota(jnp.int32, (rows, rows), 1)
    columns = []
    for b in range(n_ep):
        w = wt[b]
        share = w / jnp.sum(w, axis=0, keepdims=True)
        line = jnp.sum(jnp.where(rt[b] == z, share, 0.0), axis=0, keepdims=True)
        columns.append(jnp.sum(jnp.where(eye, jnp.broadcast_to(line, (rows, rows)), 0.0), axis=1, keepdims=True))
    column = jnp.concatenate(columns, axis=0)
    tile = 256

    def down_half(c):
        def body(t, _):
            cols = pl.ds(pl.multiple_of(c * out_cols + t * tile, tile), tile)
            acc = jnp.dot(hidden[0], full_d[0, :, cols], preferred_element_type=F32)
            for p in range(1, n_tp):
                acc = acc + jnp.dot(hidden[p], full_d[p, :, cols], preferred_element_type=F32)
            contrib[:, cols] = acc * column
            return 0

        lax.fori_loop(0, out_cols // tile, body, 0)

    down_half(0)

    def own_part(d, c):
        return contrib[
            pl.ds(pl.multiple_of(d * rows, rows), rows), pl.ds(pl.multiple_of(c * out_cols, out_cols), out_cols)
        ]

    def rl_copy(s):
        return rc(out_l.at[s], in_l.at[s], rl_s.at[s], rl_r.at[s], {"ep": z - 1})

    def rr_copy(s):
        return rc(out_r.at[s], in_r.at[s], rr_s.at[s], rr_r.at[s], {"ep": z + 1})

    def rl_got(s):
        rc(in_l.at[s], in_l.at[s], rl_s.at[s], rl_r.at[s], {"ep": z}).wait_recv()

    def rr_got(s):
        rc(in_r.at[s], in_r.at[s], rr_s.at[s], rr_r.at[s], {"ep": z}).wait_recv()

    def side(s, depth, inbox, outbox, got_fn, copy_fn, dest_fn):
        has_in = depth < last_z

        c, d = lax.div(s, last_z), lax.rem(s, last_z)
        live = jnp.logical_and(s >= 0, s < steps)

        @pl.when(jnp.logical_and(live, jnp.logical_and(has_in, d <= depth)))
        def _():
            got_fn(s)

        @pl.when(jnp.logical_and(live, d < depth))
        def _():
            mine = own_part(dest_fn(d), c)

            @pl.when(has_in)
            def _():
                outbox[s] = (mine + inbox[s].astype(F32)).astype(BF16)

            @pl.when(jnp.logical_not(has_in))
            def _():
                outbox[s] = mine.astype(BF16)

            copy_fn(s).start()

    def mixed_tile(q, _):
        cols = pl.ds(pl.multiple_of(q * tile, tile), tile)
        block = full_o.shape[1]
        acc = jnp.zeros((rows_mix, tile), F32)
        for p in range(n_tp):
            acc = acc + jnp.dot(gated[:, p * block : (p + 1) * block], full_o[p, :, cols], preferred_element_type=F32)
        mixed_ref[:, cols] = acc.astype(BF16)
        return 0

    for t in range(steps + last_z - 1):
        if t == 2:
            mate_wait(6, 7)
            down_half(1)
        if t == steps:
            mate_wait(7, n_chunks)
            own_wait(3)
            lax.fori_loop(0, width // tile, mixed_tile, 0)
        side(t - (last_z - z), z, in_l, out_l, rl_got, rl_copy, lambda b: b)
        side(t - z, last_z - z, in_r, out_r, rr_got, rr_copy, lambda b: last_z - b)
        if 7 + t <= n_chunks:
            weight_step(7 + t)

    for c in range(2):
        cols = pl.ds(c * out_cols, out_cols)
        mine = own_part(z, c)

        @pl.when(z == 0)
        def _():
            experts_ref[:, cols] = (mine + in_l[c * last_z].astype(F32)).astype(BF16)

        @pl.when(z == last_z)
        def _():
            experts_ref[:, cols] = (mine + in_r[c * last_z].astype(F32)).astype(BF16)

        @pl.when(jnp.logical_and(z > 0, z < last_z))
        def _():
            experts_ref[:, cols] = (
                mine + in_l[c * last_z + z].astype(F32) + in_r[c * last_z + last_z - z].astype(F32)
            ).astype(BF16)

    for i in range(n_chunks):
        x_copy(i).wait_send()
        y_copy(i).wait_send()
        dx_copy(i).wait_send()
        dy_copy(i).wait_send()
    for i in range(len(pieces)):
        own_copy(i).wait_send()
    for m in range(1, n_ep):
        for cp in routes_out(m):
            cp.wait_send()

    @pl.when(jnp.logical_not(is_last))
    def _():
        for cp in halo_copies():
            cp.wait_send()

    for j in range(steps):
        pl.when(jnp.logical_and(z < last_z, j < 2 * (z + 1)))(lambda j=j: zr_send(j).wait_send())
        pl.when(jnp.logical_and(z > 0, j < 2 * (last_z - z + 1)))(lambda j=j: zl_send(j).wait_send())
        pl.when(j % last_z < z)(lambda j=j: rl_copy(j).wait_send())
        pl.when(j % last_z < last_z - z)(lambda j=j: rr_copy(j).wait_send())


def per_device_fused(
    conv_x, conv_c, conv_b, conv_taps, w_out, tokens_b, norm_gain,
    route_b, route_weights, w_gate, w_up, w_down,
):
    n_ep, n_tp = lax.axis_size("ep"), lax.axis_size("tp")
    rows, width = tokens_b.shape
    rows_mix, channels = conv_x.shape
    hid = w_gate.shape[2]
    edge, half, steps = 16, rows // 2, 2 * (n_ep - 1)
    n_chunks = sum(n * sum(cols) for n, cols in CUTS)
    dma = pltpu.SemaphoreType.DMA
    hbm, vmem = pl.BlockSpec(memory_space=pl.ANY), pl.BlockSpec(memory_space=pltpu.VMEM)
    return pl.pallas_call(
        fused_kernel,
        out_shape=(
            pltpu.VMEM((rows_mix, width), BF16),
            pltpu.VMEM((rows, width), BF16),
        ),
        in_specs=[hbm, hbm, hbm, vmem, hbm, hbm, vmem, hbm, hbm, hbm, hbm, hbm],
        out_specs=(vmem, vmem),
        scratch_shapes=[
            pltpu.VMEM((n_tp,) + w_gate.shape[1:], BF16),
            pltpu.VMEM((n_tp,) + w_up.shape[1:], BF16),
            pltpu.VMEM((n_tp,) + w_down.shape[1:], BF16),
            pltpu.VMEM((n_tp,) + w_out.shape, BF16),
            pltpu.VMEM((n_ep, rows, width), BF16),
            pltpu.VMEM((n_ep * rows, width), BF16),
            pltpu.VMEM((n_ep, TOPK, rows), jnp.int32),
            pltpu.VMEM((n_ep, TOPK, rows), F32),
            pltpu.VMEM((n_tp, n_ep * rows, hid), BF16),
            pltpu.VMEM((n_ep * rows, width), F32),
        ]
        + [pltpu.VMEM((steps, rows, width // 2), BF16)] * 4
        + [pltpu.VMEM((rows_mix, channels), BF16)] * 3
        + [pltpu.VMEM((edge, channels), BF16)] * 2
        + [pltpu.VMEM((edge + rows_mix, 128), F32), pltpu.VMEM((rows_mix, channels), BF16)]
        + [dma((n_chunks,))] * 8
        + [dma((4,))] * 2
        + [dma((steps,))] * 4
        + [dma((n_ep - 1,))] * 4
        + [dma((2,))] * 2
        + [dma((steps,))] * 4
        + [dma((10,))],
        compiler_params=pltpu.CompilerParams(
            collective_id=0, has_side_effects=True, vmem_limit_bytes=54 * 1024 * 1024
        ),
    )(conv_x, conv_c, conv_b, conv_taps, w_out, tokens_b, norm_gain[None], route_b.T, route_weights.T, w_gate, w_up, w_down)


def per_device(
    conv_x,
    conv_c,
    conv_b,
    conv_taps,
    w_out,
    tokens_b,
    norm_gain,
    route_b,
    route_weights,
    w_gate,
    w_up,
    w_down,
):
    rows_mix = conv_x.shape[0]
    reach_rows = conv_taps.shape[0] - 1
    mixed_u = (conv_c.astype(jnp.float32) * conv_x.astype(jnp.float32)).astype(jnp.bfloat16)
    before = shifted(mixed_u[rows_mix - reach_rows :], ("ep", "tp"), 1)
    extended = jnp.concatenate([before, mixed_u], axis=0)
    filtered = jnp.zeros(mixed_u.shape, jnp.float32)
    for shift_tap in range(reach_rows + 1):
        filtered = filtered + conv_taps[shift_tap][None, :] * extended[
            shift_tap : shift_tap + rows_mix
        ].astype(jnp.float32)
    gated_rows = (conv_b.astype(jnp.float32) * filtered).astype(jnp.bfloat16)
    mixed_out = jnp.dot(
        gated_rows,
        lax.all_gather(w_out, "tp", axis=0, tiled=True),
        preferred_element_type=jnp.float32,
    )
    mixed_a = mixed_out.astype(jnp.bfloat16)
    tokens_f = tokens_b.astype(jnp.float32)
    normed = (
        tokens_f
        * lax.rsqrt(jnp.mean(tokens_f * tokens_f, axis=-1, keepdims=True) + 1e-06)
        * norm_gain
    ).astype(jnp.bfloat16)
    experts = lax.axis_size("ep")
    rows_exp = route_b.shape[0]
    capacity = 2 * rows_exp * TOPK // experts
    slot_total = experts * capacity
    targets = slot_targets(route_b, experts, capacity)
    weight_gate = w_gate[0]
    weight_up = w_up[0]
    weight_down = w_down[0]
    padded_rows = jnp.concatenate([normed, jnp.zeros((1, D), jnp.bfloat16)], axis=0)
    outgoing = padded_rows[fill_slots(targets, slot_total, rows_exp)]
    arrived = lax.all_to_all(outgoing, "ep", split_axis=0, concat_axis=0, tiled=True)
    hidden = expert_hidden(
        lax.all_gather(arrived, "tp", axis=0, tiled=True), weight_gate, weight_up
    )
    summed = lax.psum_scatter(
        jnp.dot(hidden, weight_down, preferred_element_type=jnp.float32).astype(jnp.bfloat16),
        "tp",
        scatter_dimension=0,
        tiled=True,
    )
    returned = lax.all_to_all(summed, "ep", split_axis=0, concat_axis=0, tiled=True)
    picked = returned[targets]
    shares = route_weights / jnp.sum(route_weights, axis=-1, keepdims=True)
    experts_b = jnp.sum(picked.astype(jnp.float32) * shares[:, :, None], axis=1).astype(
        jnp.bfloat16
    )
    return (mixed_a, experts_b)


def solution(mesh):
    dense = mesh.shape["ep"] <= 2 * TOPK and mesh.shape["tp"] == 4 and mesh.shape["grp"] == 2
    return jax.shard_map(
        per_device_fused if dense else per_device,
        mesh=mesh,
        in_specs=(
            P(("grp", "ep", "tp"), None),
            P(("grp", "ep", "tp"), None),
            P(("grp", "ep", "tp"), None),
            P(),
            P("tp", None),
            P(("grp", "ep", "tp"), None),
            P(),
            P(("grp", "ep", "tp"), None),
            P(("grp", "ep", "tp"), None),
            P("ep", None, "tp"),
            P("ep", None, "tp"),
            P("ep", "tp", None),
        ),
        out_specs=(P(("grp", "ep", "tp"), None), P(("grp", "ep", "tp"), None)),
        check_vma=False,
    )
```

```python
import functools
import jax
import jax.numpy as jnp
from jax import lax
from jax.experimental import pallas as pl
from jax.experimental.pallas import tpu as pltpu
from jax.sharding import PartitionSpec as P

D = 2048
TOPK = 2


def shifted(x, axis, by):
    size = lax.axis_size(axis)
    pairs = [(i, i + by) for i in range(size) if 0 <= i + by < size]
    return lax.ppermute(x, axis, pairs)


def slot_targets(route, experts, capacity):
    flat = route.reshape(-1)
    onehot = (flat[:, None] == jnp.arange(experts, dtype=jnp.int32)[None, :]).astype(jnp.int32)
    earlier = jnp.cumsum(onehot, axis=0) - onehot
    ranks = jnp.sum(earlier * onehot, axis=1).reshape(route.shape)
    return route * capacity + ranks


def fill_slots(targets, slot_total, filler):
    token_ids = jnp.repeat(jnp.arange(filler, dtype=jnp.int32), targets.shape[1])
    return jnp.full((slot_total,), filler, jnp.int32).at[targets.reshape(-1)].set(token_ids)


def expert_hidden(rows, weight_gate, weight_up):
    gate_val = jnp.dot(rows, weight_gate, preferred_element_type=jnp.float32)
    up_val = jnp.dot(rows, weight_up, preferred_element_type=jnp.float32)
    return (jax.nn.silu(gate_val) * up_val).astype(jnp.bfloat16)


F32 = jnp.float32
BF16 = jnp.bfloat16
CUTS = ((2, (1,)), (2, (1,)), (1, (2, 1)), (4, (1,)))


def fused_kernel(
    conv_x, conv_c, conv_b, taps, w_out, tokens, gain, route, weights, w_gate, w_up, w_down,
    mixed_ref, experts_ref,
    full_g, full_u, full_d, full_o, tok, normed, rt, wt, hidden, contrib,
    in_l, in_r, out_l, out_r, cx, cc, cb, hx, hc, ext, gated,
    x_s, x_r, y_s, y_r, dx_s, dx_r, dy_s, dy_r, own_s, own_r,
    zr_s, zr_r, zl_s, zl_r, rt_s, rt_r, wt_s, wt_r, h_s, h_r, rl_s, rl_r, rr_s, rr_r, loc,
):
    n_ep, rows, width = tok.shape
    half = rows // 2
    rows_mix = cx.shape[0]
    edge = hx.shape[0]
    last_z = n_ep - 1
    y = lax.axis_index("grp")
    z = lax.axis_index("ep")
    k = lax.axis_index("tp")
    n_tp = full_g.shape[0]
    core = lax.rem(k, 2)
    mate = k + 1 - 2 * core
    far = lax.rem(k + 2, n_tp)
    far_mate = lax.rem(mate + 2, n_tp)
    other_y = 1 - y
    flat = z * n_tp + k
    total = n_ep * n_tp
    nxt = lax.rem(flat + 1, total)
    prv = lax.rem(flat + total - 1, total)
    nxt_id = {"ep": lax.div(nxt, n_tp), "tp": lax.rem(nxt, n_tp)}
    prv_id = {"ep": lax.div(prv, n_tp), "tp": lax.rem(prv, n_tp)}

    def rc(src, dst, send, recv, dev):
        return pltpu.make_async_remote_copy(
            src_ref=src, dst_ref=dst, send_sem=send, recv_sem=recv,
            device_id=dev, device_id_type=pl.DeviceIdType.MESH,
        )

    locals_ = [
        (tokens, tok.at[z]), (route, rt.at[z]), (weights, wt.at[z]),
        (conv_x, cx), (conv_c, cc), (conv_b, cb),
        (w_gate.at[0], full_g.at[k]), (w_up.at[0], full_u.at[k]),
        (w_down.at[0], full_d.at[k]), (w_out, full_o.at[k]),
    ]
    local_copies = [pltpu.make_async_copy(a, b, loc.at[i]) for i, (a, b) in enumerate(locals_)]
    for cp in local_copies:
        cp.start()

    barrier = pltpu.get_barrier_semaphore()
    peers = [{"tp": mate}, {"tp": far}, {"grp": other_y}, nxt_id, prv_id]
    peers += [{"ep": lax.rem(z + m, n_ep)} for m in range(1, n_ep)]
    for dev in peers:
        pl.semaphore_signal(barrier, inc=1, device_id=dev, device_id_type=pl.DeviceIdType.MESH)
    pl.semaphore_wait(barrier, len(peers))

    pieces = [(w_gate.at[0], full_g), (w_up.at[0], full_u), (w_down.at[0], full_d), (w_out, full_o)]
    out_cols = full_d.shape[2] // 2
    chunks = []
    for at, (rows_cut, cols_cut) in enumerate(CUTS):
        half_rows, cols = pieces[at][1].shape[1] // 2, pieces[at][1].shape[2]
        for c, cuts in enumerate(cols_cut):
            for j in range(rows_cut * cuts):
                size = half_rows // (rows_cut * cuts)
                wide = cols // len(cols_cut)
                chunks.append((at, j * size, size, c * wide, wide))
    n_chunks = len(chunks)

    def part(i, ref, h):
        at, first, size, col, wide = chunks[i]
        start = pl.multiple_of(h * (pieces[at][1].shape[1] // 2) + first, size)
        return ref.at[pl.ds(start, size), pl.ds(col, wide)]

    def full_at(i, piece, h):
        return part(i, pieces[chunks[i][0]][1].at[piece], h)

    def x_copy(i):
        return rc(part(i, pieces[chunks[i][0]][0], y), full_at(i, k, y), x_s.at[i], x_r.at[i], {"tp": far})

    def y_copy(i):
        at = full_at(i, far, y)
        return rc(at, at, y_s.at[i], y_r.at[i], {"grp": other_y})

    def dx_copy(i):
        at = full_at(i, far, y)
        return rc(at, at, dx_s.at[i], dx_r.at[i], {"tp": mate})

    def dy_copy(i):
        at = full_at(i, far, other_y)
        return rc(at, at, dy_s.at[i], dy_r.at[i], {"tp": mate})

    def own_copy(i):
        own, full = pieces[i]
        return rc(own, full.at[k], own_s.at[i], own_r.at[i], {"tp": mate})

    def got(i, piece, h, send, recv):
        at = full_at(i, piece, h)
        rc(at, at, send.at[i], recv.at[i], {"tp": mate}).wait_recv()

    rows_of = lambda j: pl.ds((j % 2) * half, half)

    def zr_send(j):
        b = z - j // 2
        src = tokens.at[rows_of(j)] if j < 2 else tok.at[b, rows_of(j)]
        return rc(src, tok.at[b, rows_of(j)], zr_s.at[j], zr_r.at[j], {"ep": z + 1})

    def zl_send(j):
        b = z + j // 2
        src = tokens.at[rows_of(j)] if j < 2 else tok.at[b, rows_of(j)]
        return rc(src, tok.at[b, rows_of(j)], zl_s.at[j], zl_r.at[j], {"ep": z - 1})

    def zr_got(j):
        at = tok.at[z - 1 - j // 2, rows_of(j)]
        rc(at, at, zr_s.at[j], zr_r.at[j], {"ep": z - 1}).wait_recv()

    def zl_got(j):
        at = tok.at[z + 1 + j // 2, rows_of(j)]
        rc(at, at, zl_s.at[j], zl_r.at[j], {"ep": z + 1}).wait_recv()

    def route_copies(m, here, there):
        dev = {"ep": there}
        return (
            rc(route, rt.at[here], rt_s.at[m - 1], rt_r.at[m - 1], dev),
            rc(weights, wt.at[here], wt_s.at[m - 1], wt_r.at[m - 1], dev),
        )

    def routes_out(m):
        return route_copies(m, z, lax.rem(z + m, n_ep))

    tail = pl.ds(rows_mix - edge, edge)

    def halo_copies():
        return (
            rc(conv_x.at[tail], hx, h_s.at[0], h_r.at[0], nxt_id),
            rc(conv_c.at[tail], hc, h_s.at[1], h_r.at[1], nxt_id),
        )

    is_first, is_last = flat == 0, flat == total - 1

    for m in range(1, n_ep):
        for cp in routes_out(m):
            cp.start()

    @pl.when(jnp.logical_not(is_last))
    def _():
        for cp in halo_copies():
            cp.start()

    for j in range(2):
        pl.when(z < last_z)(lambda j=j: zr_send(j).start())
        pl.when(z > 0)(lambda j=j: zl_send(j).start())
    for i in range(n_chunks):
        x_copy(i).start()
    for i in range(len(pieces)):
        own_copy(i).start()
    for cp in local_copies:
        cp.wait()

    @pl.when(is_first)
    def _():
        hx[...] = jnp.zeros_like(hx)
        hc[...] = jnp.zeros_like(hc)

    @pl.when(jnp.logical_not(is_first))
    def _():
        for cp in halo_copies():
            cp.wait_recv()

    n_taps = taps.shape[0]

    def conv_tile(t, _):
        cols = pl.ds(pl.multiple_of(t * 128, 128), 128)
        ext[pl.ds(0, edge), :] = (hc[:, cols].astype(F32) * hx[:, cols].astype(F32)).astype(BF16).astype(F32)
        ext[pl.ds(edge, rows_mix), :] = (cc[:, cols].astype(F32) * cx[:, cols].astype(F32)).astype(BF16).astype(F32)
        filtered = jnp.zeros((rows_mix, 128), F32)
        for s in range(n_taps):
            filtered = filtered + taps[pl.ds(s, 1), cols] * ext[pl.ds(edge - (n_taps - 1) + s, rows_mix), :]
        gated[:, cols] = (cb[:, cols].astype(F32) * filtered).astype(BF16)
        return 0

    lax.fori_loop(0, cx.shape[1] // 128, conv_tile, 0)

    def norm_block(b):
        def body(r, _):
            at = pl.ds(pl.multiple_of(r * 32, 32), 32)
            v = tok[b, at, :].astype(F32)
            scale = lax.rsqrt(jnp.mean(v * v, axis=-1, keepdims=True) + 1e-06)
            normed[pl.ds(pl.multiple_of(b * rows + r * 32, 32), 32), :] = (v * scale * gain[...]).astype(BF16)
            return 0

        lax.fori_loop(0, rows // 32, body, 0)

    first_near = k - core
    first_far = n_tp - 2 - first_near

    def hidden_of(p, at):
        g = jnp.dot(normed[at, :], full_g[p], preferred_element_type=F32)
        u = jnp.dot(normed[at, :], full_u[p], preferred_element_type=F32)
        hidden[p, at, :] = (jax.nn.silu(g) * u).astype(BF16)

    def near_block(b):
        norm_block(b)
        at = pl.ds(pl.multiple_of(b * rows, rows), rows)

        def body(m, _):
            hidden_of(first_near + m, at)
            return 0

        lax.fori_loop(0, 2, body, 0)

    def weight_step(i, with_y=True, with_x=True):
        if with_x and i < n_chunks:
            got(i, far, y, x_s, x_r)
            y_copy(i).start()
            dx_copy(i).start()
        if with_y and 1 <= i <= n_chunks:
            got(i - 1, far, other_y, y_s, y_r)
            dy_copy(i - 1).start()

    def mate_wait(lo, hi):
        for i in range(lo, hi):
            got(i, far_mate, y, dx_s, dx_r)
            got(i, far_mate, other_y, dy_s, dy_r)

    def own_wait(i):
        at = pieces[i][1].at[mate]
        rc(at, at, own_s.at[i], own_r.at[i], {"tp": mate}).wait_recv()

    own_wait(0)
    own_wait(1)
    near_block(z)

    steps = 2 * last_z
    for s in range(steps):
        @pl.when(s < 2 * z)
        def _():
            zr_got(s)
            if s + 2 < steps:
                pl.when(z < last_z)(lambda: zr_send(s + 2).start())

        @pl.when(s < 2 * (last_z - z))
        def _():
            zl_got(s)
            if s + 2 < steps:
                pl.when(z > 0)(lambda: zl_send(s + 2).start())

        weight_step(s)
        if s % 2 == 1:
            m = s // 2 + 1
            pl.when(z - m >= 0)(lambda: near_block(z - m))
        m = s // 2 if s % 2 == 0 else (last_z if s == steps - 1 else 0)
        if m:
            pl.when(z + m <= last_z)(lambda: near_block(z + m))

    mate_wait(0, 4)

    def far_piece(m, _):
        hidden_of(first_far + m, pl.ds(0, n_ep * rows))
        return 0

    lax.fori_loop(0, 2, far_piece, 0)
    weight_step(6, with_x=False)
    weight_step(6, with_y=False)
    mate_wait(4, 6)
    own_wait(2)
    for m in range(1, n_ep):
        for cp in route_copies(m, lax.rem(z + n_ep - m, n_ep), z):
            cp.wait_recv()

    eye = lax.broadcasted_iota(jnp.int32, (rows, rows), 0) == lax.broadcasted_iota(jnp.int32, (rows, rows), 1)
    columns = []
    for b in range(n_ep):
        w = wt[b]
        share = w / jnp.sum(w, axis=0, keepdims=True)
        line = jnp.sum(jnp.where(rt[b] == z, share, 0.0), axis=0, keepdims=True)
        columns.append(jnp.sum(jnp.where(eye, jnp.broadcast_to(line, (rows, rows)), 0.0), axis=1, keepdims=True))
    column = jnp.concatenate(columns, axis=0)
    tile = 256

    def down_half(c):
        def body(t, _):
            cols = pl.ds(pl.multiple_of(c * out_cols + t * tile, tile), tile)
            acc = jnp.dot(hidden[0], full_d[0, :, cols], preferred_element_type=F32)
            for p in range(1, n_tp):
                acc = acc + jnp.dot(hidden[p], full_d[p, :, cols], preferred_element_type=F32)
            contrib[:, cols] = acc * column
            return 0

        lax.fori_loop(0, out_cols // tile, body, 0)

    down_half(0)

    def own_part(d, c):
        return contrib[
            pl.ds(pl.multiple_of(d * rows, rows), rows), pl.ds(pl.multiple_of(c * out_cols, out_cols), out_cols)
        ]

    def rl_copy(s):
        return rc(out_l.at[s], in_l.at[s], rl_s.at[s], rl_r.at[s], {"ep": z - 1})

    def rr_copy(s):
        return rc(out_r.at[s], in_r.at[s], rr_s.at[s], rr_r.at[s], {"ep": z + 1})

    def rl_got(s):
        rc(in_l.at[s], in_l.at[s], rl_s.at[s], rl_r.at[s], {"ep": z}).wait_recv()

    def rr_got(s):
        rc(in_r.at[s], in_r.at[s], rr_s.at[s], rr_r.at[s], {"ep": z}).wait_recv()

    def side(s, depth, inbox, outbox, got_fn, copy_fn, dest_fn):
        has_in = depth < last_z

        c, d = lax.div(s, last_z), lax.rem(s, last_z)
        live = jnp.logical_and(s >= 0, s < steps)

        @pl.when(jnp.logical_and(live, d < depth))
        def _():
            mine = own_part(dest_fn(d), c)

            @pl.when(has_in)
            def _():
                got_fn(s)
                outbox[s] = (mine + inbox[s].astype(F32)).astype(BF16)

            @pl.when(jnp.logical_not(has_in))
            def _():
                outbox[s] = mine.astype(BF16)

            copy_fn(s).start()

    def mixed_tile(q, _):
        cols = pl.ds(pl.multiple_of(q * tile, tile), tile)
        block = full_o.shape[1]
        acc = jnp.zeros((rows_mix, tile), F32)
        for p in range(n_tp):
            acc = acc + jnp.dot(gated[:, p * block : (p + 1) * block], full_o[p, :, cols], preferred_element_type=F32)
        mixed_ref[:, cols] = acc.astype(BF16)
        return 0

    for t in range(steps + last_z - 1):
        if t == 2:
            mate_wait(6, 7)
            down_half(1)
        if t == steps:
            mate_wait(7, n_chunks)
            own_wait(3)
            lax.fori_loop(0, width // tile, mixed_tile, 0)
        side(t - (last_z - z), z, in_l, out_l, rl_got, rl_copy, lambda b: b)
        side(t - z, last_z - z, in_r, out_r, rr_got, rr_copy, lambda b: last_z - b)
        if 7 + t <= n_chunks:
            weight_step(7 + t)

    for c in range(2):
        cols = pl.ds(c * out_cols, out_cols)
        mine = own_part(z, c)

        pl.when(z < last_z)(lambda: rl_got(c * last_z + z))
        pl.when(z > 0)(lambda: rr_got(c * last_z + last_z - z))

        @pl.when(z == 0)
        def _():
            experts_ref[:, cols] = (mine + in_l[c * last_z].astype(F32)).astype(BF16)

        @pl.when(z == last_z)
        def _():
            experts_ref[:, cols] = (mine + in_r[c * last_z].astype(F32)).astype(BF16)

        @pl.when(jnp.logical_and(z > 0, z < last_z))
        def _():
            experts_ref[:, cols] = (
                mine + in_l[c * last_z + z].astype(F32) + in_r[c * last_z + last_z - z].astype(F32)
            ).astype(BF16)

    for i in range(n_chunks):
        x_copy(i).wait_send()
        y_copy(i).wait_send()
        dx_copy(i).wait_send()
        dy_copy(i).wait_send()
    for i in range(len(pieces)):
        own_copy(i).wait_send()
    for m in range(1, n_ep):
        for cp in routes_out(m):
            cp.wait_send()

    @pl.when(jnp.logical_not(is_last))
    def _():
        for cp in halo_copies():
            cp.wait_send()

    for j in range(steps):
        pl.when(jnp.logical_and(z < last_z, j < 2 * (z + 1)))(lambda j=j: zr_send(j).wait_send())
        pl.when(jnp.logical_and(z > 0, j < 2 * (last_z - z + 1)))(lambda j=j: zl_send(j).wait_send())
        pl.when(j % last_z < z)(lambda j=j: rl_copy(j).wait_send())
        pl.when(j % last_z < last_z - z)(lambda j=j: rr_copy(j).wait_send())


def per_device_fused(
    conv_x, conv_c, conv_b, conv_taps, w_out, tokens_b, norm_gain,
    route_b, route_weights, w_gate, w_up, w_down,
):
    n_ep, n_tp = lax.axis_size("ep"), lax.axis_size("tp")
    rows, width = tokens_b.shape
    rows_mix, channels = conv_x.shape
    hid = w_gate.shape[2]
    edge, half, steps = 16, rows // 2, 2 * (n_ep - 1)
    n_chunks = sum(n * sum(cols) for n, cols in CUTS)
    dma = pltpu.SemaphoreType.DMA
    hbm, vmem = pl.BlockSpec(memory_space=pl.ANY), pl.BlockSpec(memory_space=pltpu.VMEM)
    return pl.pallas_call(
        fused_kernel,
        out_shape=(
            pltpu.VMEM((rows_mix, width), BF16),
            pltpu.VMEM((rows, width), BF16),
        ),
        in_specs=[hbm, hbm, hbm, vmem, hbm, hbm, vmem, hbm, hbm, hbm, hbm, hbm],
        out_specs=(vmem, vmem),
        scratch_shapes=[
            pltpu.VMEM((n_tp,) + w_gate.shape[1:], BF16),
            pltpu.VMEM((n_tp,) + w_up.shape[1:], BF16),
            pltpu.VMEM((n_tp,) + w_down.shape[1:], BF16),
            pltpu.VMEM((n_tp,) + w_out.shape, BF16),
            pltpu.VMEM((n_ep, rows, width), BF16),
            pltpu.VMEM((n_ep * rows, width), BF16),
            pltpu.VMEM((n_ep, TOPK, rows), jnp.int32),
            pltpu.VMEM((n_ep, TOPK, rows), F32),
            pltpu.VMEM((n_tp, n_ep * rows, hid), BF16),
            pltpu.VMEM((n_ep * rows, width), F32),
        ]
        + [pltpu.VMEM((steps, rows, width // 2), BF16)] * 4
        + [pltpu.VMEM((rows_mix, channels), BF16)] * 3
        + [pltpu.VMEM((edge, channels), BF16)] * 2
        + [pltpu.VMEM((edge + rows_mix, 128), F32), pltpu.VMEM((rows_mix, channels), BF16)]
        + [dma((n_chunks,))] * 8
        + [dma((4,))] * 2
        + [dma((steps,))] * 4
        + [dma((n_ep - 1,))] * 4
        + [dma((2,))] * 2
        + [dma((steps,))] * 4
        + [dma((10,))],
        compiler_params=pltpu.CompilerParams(
            collective_id=0, has_side_effects=True, vmem_limit_bytes=54 * 1024 * 1024
        ),
    )(conv_x, conv_c, conv_b, conv_taps, w_out, tokens_b, norm_gain[None], route_b.T, route_weights.T, w_gate, w_up, w_down)


def per_device(
    conv_x,
    conv_c,
    conv_b,
    conv_taps,
    w_out,
    tokens_b,
    norm_gain,
    route_b,
    route_weights,
    w_gate,
    w_up,
    w_down,
):
    rows_mix = conv_x.shape[0]
    reach_rows = conv_taps.shape[0] - 1
    mixed_u = (conv_c.astype(jnp.float32) * conv_x.astype(jnp.float32)).astype(jnp.bfloat16)
    before = shifted(mixed_u[rows_mix - reach_rows :], ("ep", "tp"), 1)
    extended = jnp.concatenate([before, mixed_u], axis=0)
    filtered = jnp.zeros(mixed_u.shape, jnp.float32)
    for shift_tap in range(reach_rows + 1):
        filtered = filtered + conv_taps[shift_tap][None, :] * extended[
            shift_tap : shift_tap + rows_mix
        ].astype(jnp.float32)
    gated_rows = (conv_b.astype(jnp.float32) * filtered).astype(jnp.bfloat16)
    mixed_out = jnp.dot(
        gated_rows,
        lax.all_gather(w_out, "tp", axis=0, tiled=True),
        preferred_element_type=jnp.float32,
    )
    mixed_a = mixed_out.astype(jnp.bfloat16)
    tokens_f = tokens_b.astype(jnp.float32)
    normed = (
        tokens_f
        * lax.rsqrt(jnp.mean(tokens_f * tokens_f, axis=-1, keepdims=True) + 1e-06)
        * norm_gain
    ).astype(jnp.bfloat16)
    experts = lax.axis_size("ep")
    rows_exp = route_b.shape[0]
    capacity = 2 * rows_exp * TOPK // experts
    slot_total = experts * capacity
    targets = slot_targets(route_b, experts, capacity)
    weight_gate = w_gate[0]
    weight_up = w_up[0]
    weight_down = w_down[0]
    padded_rows = jnp.concatenate([normed, jnp.zeros((1, D), jnp.bfloat16)], axis=0)
    outgoing = padded_rows[fill_slots(targets, slot_total, rows_exp)]
    arrived = lax.all_to_all(outgoing, "ep", split_axis=0, concat_axis=0, tiled=True)
    hidden = expert_hidden(
        lax.all_gather(arrived, "tp", axis=0, tiled=True), weight_gate, weight_up
    )
    summed = lax.psum_scatter(
        jnp.dot(hidden, weight_down, preferred_element_type=jnp.float32).astype(jnp.bfloat16),
        "tp",
        scatter_dimension=0,
        tiled=True,
    )
    returned = lax.all_to_all(summed, "ep", split_axis=0, concat_axis=0, tiled=True)
    picked = returned[targets]
    shares = route_weights / jnp.sum(route_weights, axis=-1, keepdims=True)
    experts_b = jnp.sum(picked.astype(jnp.float32) * shares[:, :, None], axis=1).astype(
        jnp.bfloat16
    )
    return (mixed_a, experts_b)


def solution(mesh):
    dense = mesh.shape["ep"] <= 2 * TOPK and mesh.shape["tp"] == 4 and mesh.shape["grp"] == 2
    return jax.shard_map(
        per_device_fused if dense else per_device,
        mesh=mesh,
        in_specs=(
            P(("grp", "ep", "tp"), None),
            P(("grp", "ep", "tp"), None),
            P(("grp", "ep", "tp"), None),
            P(),
            P("tp", None),
            P(("grp", "ep", "tp"), None),
            P(),
            P(("grp", "ep", "tp"), None),
            P(("grp", "ep", "tp"), None),
            P("ep", None, "tp"),
            P("ep", None, "tp"),
            P("ep", "tp", None),
        ),
        out_specs=(P(("grp", "ep", "tp"), None), P(("grp", "ep", "tp"), None)),
        check_vma=False,
    )
```
